512 devices in a mesh: sp: 64 (over z, y), tp: 8 (over x, core).
Axes of the slice: x: 4, y: 4, z: 16, core: 2. Of those that a mesh axis runs over, the one named last changes fastest.
Arguments:
- query_heads: bfloat16 [8192, 1024], P('sp', 'tp'), may hold values from -12 to 12
- key_heads: bfloat16 [8192, 1024], P('sp', 'tp'), may hold values from -6 to 6
- value_heads: bfloat16 [8192, 1024], P('sp', 'tp'), may hold values from -6 to 6
- decay_sums: float32 [8192, 8], P('sp', 'tp'), may hold values from -1346 to 0, as said below
- row_logsums: float32 [8192, 8], P('sp', 'tp'), may hold values from -9216 to 17408, as said below
- head_outputs: bfloat16 [8192, 1024], P('sp', 'tp'), may hold values from -1.796875 to 1.796875
- out_cotangent: bfloat16 [8192, 1024], P('sp', 'tp'), may hold values from -64 to 64
- normed_input: bfloat16 [8192, 2048], P('sp', 'tp'), may hold values from -16 to 16
Outputs:
- query_grads: bfloat16 [8192, 1024], P('sp', 'tp')
- key_grads: bfloat16 [8192, 1024], P('sp', 'tp')
- value_grads: bfloat16 [8192, 1024], P('sp', 'tp')
- weight_grad: float32 [2048, 1024], P('sp', 'tp')
The draws below stay inside these ranges and needn't reach their ends.
Inputs may be any that keep to these rules, and one draw needn't show every extreme that they name: `decay_sums`: each head's values never rise along the positions. `row_logsums`: each entry is the logarithm of the sum, over key positions up to the row's own, of the exponentials of score_scale times the inner product plus the gate difference, as in the reference program.
All inputs are finite; a program needn't handle non-finite values.
Results may differ from the reference program's by a relative error of at most 0.005.
Values may be sent and summed in bfloat16 or wider, within the bound.
No kernel may reach another device: no remote copies, remote signals or barrier semaphores. Data moves between devices by JAX's collectives and lax.ppermute only.
A program may use at most 64 MiB of HBM per device.

```python
import jax
import jax.numpy as jnp
from jax import lax

D = 2048
HEAD_TOTAL = 8
HEAD_SIZE = 128
TOK_DEV = 128
TOKEN_TOTAL = 8192


def head_inputs(key):
    queries = jax.random.normal(jax.random.fold_in(key, 11), (TOKEN_TOTAL, HEAD_TOTAL * HEAD_SIZE), jnp.float32)
    keys_drawn = jax.random.normal(jax.random.fold_in(key, 12), (TOKEN_TOTAL, HEAD_TOTAL * HEAD_SIZE), jnp.float32)
    queries = jnp.clip(queries, -6.0, 6.0)
    keys_drawn = jnp.clip(keys_drawn, -6.0, 6.0)
    return (queries.astype(jnp.bfloat16), keys_drawn.astype(jnp.bfloat16))


def gate_totals(key):
    order = jax.random.permutation(jax.random.fold_in(key, 21), HEAD_TOTAL)
    fast_count = HEAD_TOTAL // 2
    fast = order < fast_count
    slow_rate = jnp.exp(jax.random.uniform(jax.random.fold_in(key, 22), (HEAD_TOTAL,), jnp.float32, -1.204, -0.223)) / TOKEN_TOTAL
    fast_rate = jnp.exp(jax.random.uniform(jax.random.fold_in(key, 23), (HEAD_TOTAL,), jnp.float32, 0.693, 1.792)) / TOK_DEV
    rate = jnp.where(fast, fast_rate, slow_rate)
    block_factor = jnp.exp(jax.random.uniform(jax.random.fold_in(key, 24), (TOKEN_TOTAL // TOK_DEV, 1, HEAD_TOTAL), jnp.float32, -0.693, 0.693))
    position_factor = jax.random.uniform(jax.random.fold_in(key, 25), (TOKEN_TOTAL // TOK_DEV, TOK_DEV, HEAD_TOTAL), jnp.float32, 0.3, 1.7)
    step_amount = (rate * block_factor * position_factor).reshape(TOKEN_TOTAL, HEAD_TOTAL)
    spike_location = jax.random.randint(jax.random.fold_in(key, 26), (2, 1, HEAD_TOTAL), 0, TOKEN_TOTAL)
    spike_penalty = -jnp.log(1.0 - jax.random.uniform(jax.random.fold_in(key, 27), (2, 1, HEAD_TOTAL), jnp.float32, 0.2, 0.4))
    token_places = jnp.arange(TOKEN_TOTAL, dtype=jnp.int32)[None, :, None]
    spike_events = jnp.sum(jnp.where(token_places == spike_location, spike_penalty, 0.0), axis=0)
    return jnp.cumsum(-(step_amount + spike_events), axis=0)


def draw_query_heads(key, part):
    return head_inputs(key)[0]


def draw_key_heads(key, part):
    return head_inputs(key)[1]


def draw_decay_sums(key, part):
    return gate_totals(key)


def draw_row_logsums(key, part):
    queries, keys_drawn = head_inputs(key)
    gates = gate_totals(key)
    query_rows = queries.astype(jnp.float32).reshape(TOKEN_TOTAL, HEAD_TOTAL, HEAD_SIZE)
    key_rows = keys_drawn.astype(jnp.float32).reshape(TOKEN_TOTAL, HEAD_TOTAL, HEAD_SIZE)
    length = TOKEN_TOTAL
    while length > 256 and length % 2 == 0:
        length = length // 2
    token_places = jnp.arange(TOKEN_TOTAL, dtype=jnp.int32)

    def one_block(first_row):
        query_part = lax.dynamic_slice_in_dim(query_rows, first_row, length, 0)
        gate_part = lax.dynamic_slice_in_dim(gates, first_row, length, 0)
        scores = jnp.einsum('ahd,bhd->hab', query_part, key_rows) * HEAD_SIZE ** (-0.5)
        scores = scores + (gate_part.T[:, :, None] - gates.T[:, None, :])
        query_pos = first_row + jnp.arange(length, dtype=jnp.int32)
        allowed = token_places[None, None, :] <= query_pos[None, :, None]
        scores = jnp.where(allowed, scores, -jnp.inf)
        return jax.nn.logsumexp(scores, axis=2).T
    blocks = lax.map(one_block, jnp.arange(TOKEN_TOTAL // length, dtype=jnp.int32) * length)
    return blocks.reshape(TOKEN_TOTAL, HEAD_TOTAL)


def raised(values, stream_key, source, target, blocks, factor):
    def block_of(dim):
        return (jnp.arange(values.shape[dim]) // (values.shape[dim] // blocks)).reshape((-1,) + (1,) * (values.ndim - 1 - dim))

    near = jax.random.permutation(stream_key, blocks)[block_of(target)]
    second = (block_of(target) + blocks // 2) % blocks
    return jnp.where((block_of(source) == near) | (block_of(source) == second), factor * values, values)


def block_levels(own_key, extent, cuts, smallest, top_value):
    def one(position, parts):
        heights = jax.random.uniform(jax.random.fold_in(jax.random.fold_in(own_key, 6), position), (parts,), jnp.float32, smallest / len(cuts), top_value / len(cuts))
        return jnp.repeat(jnp.exp(heights), extent[position] // parts).reshape((-1,) + (1,) * (len(extent) - position - 1))

    gain = one(*cuts[0])
    for cut in cuts[1:]:
        gain = gain * one(*cut)
    return gain


def centred(stream_key, shape, spread, limit, pieces=(), held_as=jnp.bfloat16):
    result = spread * jax.random.normal(stream_key, shape, jnp.float32)
    if pieces:
        result = result * block_levels(stream_key, shape, pieces, -0.22, 0.18)
    return jnp.clip(result, -limit, limit).astype(held_as)


def heavy_noise(rng, extent, scale, bound, cuts, heavy, kind=jnp.bfloat16):
    values = scale * jax.random.normal(rng, extent, jnp.float32)
    if cuts:
        values = values * block_levels(rng, extent, cuts, -0.22, 0.18)
    return jnp.clip(raised(values, jax.random.fold_in(rng, 3), *heavy), -bound, bound).astype(kind)


def setup_inputs(seed: int = 0) -> dict:
    seeds = jax.random.split(jax.random.key(seed), 9)
    query_heads = draw_query_heads(jax.random.fold_in(seeds[8], 71), 0)
    key_heads = draw_key_heads(jax.random.fold_in(seeds[8], 71), 0)
    value_heads = centred(seeds[2], (TOKEN_TOTAL, HEAD_TOTAL * HEAD_SIZE), 1.0, 6.0, ((0, 64), (1, 8)))
    decay_sums = draw_decay_sums(jax.random.fold_in(seeds[8], 71), 0)
    row_logsums = draw_row_logsums(jax.random.fold_in(seeds[8], 71), 0)
    head_outputs = centred(seeds[5], (TOKEN_TOTAL, HEAD_TOTAL * HEAD_SIZE), 0.3, 1.796875, ((0, 64), (1, 8)))
    out_cotangent = heavy_noise(seeds[6], (TOKEN_TOTAL, HEAD_TOTAL * HEAD_SIZE), 4.0, 64.0, ((0, 64), (1, 8)), (0, 1, 64, 4.0))
    normed_input = heavy_noise(seeds[7], (TOKEN_TOTAL, D), 1.0, 16.0, ((0, 64), (1, 8)), (0, 1, 64, 4.0))
    return {"query_heads": query_heads, "key_heads": key_heads, "value_heads": value_heads, "decay_sums": decay_sums, "row_logsums": row_logsums, "head_outputs": head_outputs, "out_cotangent": out_cotangent, "normed_input": normed_input}


def rounded(values):
    return lax.optimization_barrier(values.astype(jnp.bfloat16)).astype(jnp.float32)


def reference(query_heads, key_heads, value_heads, decay_sums, row_logsums, head_outputs, out_cotangent, normed_input):
    token_count, row_width = query_heads.shape
    head_count = decay_sums.shape[1]
    head_width = row_width // head_count
    score_scale = head_width ** -0.5
    shape = (token_count, head_count, head_width)
    queries_all = query_heads.astype(jnp.float32).reshape(shape)
    keys_all = key_heads.astype(jnp.float32).reshape(shape)
    values_all = value_heads.astype(jnp.float32).reshape(shape)
    grads_all = out_cotangent.astype(jnp.float32).reshape(shape)
    outputs_all = head_outputs.astype(jnp.float32).reshape(shape)
    row_terms = jnp.sum(outputs_all * grads_all, axis=2)
    token_places = jnp.arange(token_count, dtype=jnp.int32)
    length = token_count
    while length > 256 and length % 2 == 0:
        length = length // 2
    number = token_count // length

    def visit_one(running, first_row):
        key_sum, value_sum = running
        query_part = lax.dynamic_slice_in_dim(queries_all, first_row, length, 0)
        grad_part = lax.dynamic_slice_in_dim(grads_all, first_row, length, 0)
        gate_part = lax.dynamic_slice_in_dim(decay_sums, first_row, length, 0)
        norm_part = lax.dynamic_slice_in_dim(row_logsums, first_row, length, 0)
        term_part = lax.dynamic_slice_in_dim(row_terms, first_row, length, 0)
        query_pos = first_row + jnp.arange(length, dtype=jnp.int32)
        scores = jnp.einsum("ahd,bhd->hab", query_part, keys_all) * score_scale
        scores = scores + (gate_part.T[:, :, None] - decay_sums.T[:, None, :])
        allowed = token_places[None, None, :] <= query_pos[None, :, None]
        weights = jnp.exp(jnp.where(allowed, scores - norm_part.T[:, :, None], -jnp.inf))
        flows = jnp.einsum("ahd,bhd->hab", grad_part, values_all)
        slopes = weights * (flows - term_part.T[:, :, None])
        slopes_low = rounded(slopes)
        weights_low = rounded(weights)
        query_block = (jnp.einsum("hab,bhd->ahd", slopes_low, keys_all) * score_scale).astype(jnp.bfloat16)
        key_sum = key_sum + jnp.einsum("hab,ahd->bhd", slopes_low, query_part)
        value_sum = value_sum + jnp.einsum("hab,ahd->bhd", weights_low, grad_part)
        return (key_sum, value_sum), query_block

    zero_sums = jnp.zeros(shape, jnp.float32)
    starts = jnp.arange(number, dtype=jnp.int32) * length
    (key_sum, value_sum), query_blocks = lax.scan(visit_one, (zero_sums, zero_sums), starts)
    query_grads = query_blocks.reshape(token_count, row_width)
    key_grads = (key_sum * score_scale).astype(jnp.bfloat16).reshape(token_count, row_width)
    value_grads = value_sum.astype(jnp.bfloat16).reshape(token_count, row_width)
    weight_grad = jnp.dot(normed_input.T, query_grads, preferred_element_type=jnp.float32)
    return query_grads, key_grads, value_grads, weight_grad
```

```python
import functools

import jax
import jax.numpy as jnp
from jax import lax
from jax.experimental import pallas as pl
from jax.experimental.pallas import tpu as pltpu
from jax.sharding import Mesh
from jax.sharding import PartitionSpec as P

SP = ("z", "y")
TP = ("x", "c")
NZ, NY, NX, NC = 16, 4, 4, 2
T = 128
H = 128
SCALE = H**-0.5
ZB = 2 * T + 8
YB = 4 * T + 16
RB = 4 * T + 2 * T
f32 = jnp.float32
bf16 = jnp.bfloat16


def nt(a, b):
    return lax.dot_general(a, b, (((1,), (1,)), ((), ())), preferred_element_type=f32)


def nn(a, b):
    return lax.dot_general(a, b, (((1,), (0,)), ((), ())), preferred_element_type=f32)


def three(x):
    hi = x.astype(bf16)
    rest = x - hi.astype(f32)
    mid = rest.astype(bf16)
    low = (rest - mid.astype(f32)).astype(bf16)
    return [hi, mid, low]


def pack_body(place, q, k, v, g, lse, o, do, zsend, own):
    z = place[0]
    terms = o[...].astype(f32) * do[...].astype(f32)
    r = jnp.sum(terms.T, axis=0, keepdims=True)
    gate = g[...]
    a = gate - lse[...]
    zero = jnp.zeros((1, T), bf16)
    q_stats = three(a) + three(r)
    k_stats = three(gate)
    q_rows = jnp.concatenate(q_stats + [zero, zero], axis=0)
    k_rows = jnp.concatenate(k_stats + [zero] * 5, axis=0)
    own[0:T] = q[...]
    own[T : 2 * T] = do[...]
    own[2 * T : 3 * T] = k[...]
    own[3 * T : 4 * T] = v[...]
    own[4 * T : YB] = jnp.concatenate(q_stats + k_stats + [zero] * 7, axis=0)

    def one(j, carry):
        @pl.when(j > z)
        def _():
            zsend[j, 0:T] = k[...]
            zsend[j, T : 2 * T] = v[...]
            zsend[j, 2 * T : ZB] = k_rows

        @pl.when(j <= z)
        def _():
            zsend[j, 0:T] = q[...]
            zsend[j, T : 2 * T] = do[...]
            zsend[j, 2 * T : ZB] = q_rows

        return carry

    lax.fori_loop(0, NZ, one, 0)


def joined(rows):
    w = rows.astype(f32)
    return w[0:1] + w[1:2] + w[2:3]


def upright(row):
    i = lax.broadcasted_iota(jnp.int32, (T, T), 0)
    j = lax.broadcasted_iota(jnp.int32, (T, T), 1)
    return jnp.sum(jnp.where(i == j, row, 0.0), axis=1, keepdims=True)


def attend_body(place, recv, grp, ysend, dq, dk, dv):
    z = place[0]
    y = place[1]
    qg = jnp.concatenate([grp[i, 0:T] for i in range(NY)], axis=0)
    dog = jnp.concatenate([grp[i, T : 2 * T] for i in range(NY)], axis=0)
    kg = jnp.concatenate([grp[i, 2 * T : 3 * T] for i in range(NY)], axis=0)
    vg = jnp.concatenate([grp[i, 3 * T : 4 * T] for i in range(NY)], axis=0)
    stats = [grp[i, 4 * T : YB] for i in range(NY)]
    a_col = jnp.concatenate([upright(joined(s[0:3])) for s in stats], axis=0)
    r_col = jnp.concatenate([upright(joined(s[3:6])) for s in stats], axis=0)
    g_col = jnp.concatenate([upright(joined(s[6:9])) for s in stats], axis=0)

    def query_part(k, v, g_row, mask):
        s = nt(qg, k) * SCALE + (a_col - g_row)
        if mask is not None:
            s = jnp.where(mask, s, -jnp.inf)
        w = jnp.exp(s)
        sl = (w * (nt(dog, v) - r_col)).astype(bf16)
        return nn(sl, k)

    def key_part(q, do, a_row, r_row, mask):
        s = nt(kg, q) * SCALE + (a_row - g_col)
        if mask is not None:
            s = jnp.where(mask, s, -jnp.inf)
        w = jnp.exp(s)
        sl = (w * (nt(vg, do) - r_row)).astype(bf16)
        return nn(sl, q), nn(w.astype(bf16), do)

    big = lax.broadcasted_iota(jnp.int32, (NY * T, T), 0)
    small = lax.broadcasted_iota(jnp.int32, (NY * T, T), 1) + y * T
    own_stats = grp[y, 4 * T : YB]
    dq[...] = query_part(grp[y, 2 * T : 3 * T], grp[y, 3 * T : 4 * T], joined(own_stats[6:9]), small <= big)
    first = key_part(
        grp[y, 0:T], grp[y, T : 2 * T], joined(own_stats[0:3]), joined(own_stats[3:6]), big <= small
    )
    dk[...] = first[0]
    dv[...] = first[1]

    def below(j, carry):
        dq[...] += query_part(recv[j, 0:T], recv[j, T : 2 * T], joined(recv[j, 2 * T : ZB][0:3]), None)
        return carry

    def above(j, carry):
        rows = recv[j, 2 * T : ZB]
        more = key_part(recv[j, 0:T], recv[j, T : 2 * T], joined(rows[0:3]), joined(rows[3:6]), None)
        dk[...] += more[0]
        dv[...] += more[1]
        return carry

    lax.fori_loop(0, z, below, 0)
    lax.fori_loop(z + 1, NZ, above, 0)
    sums = dq[...].astype(bf16)
    for i in range(NY):
        ysend[i, 0 : 4 * T] = sums
        ysend[i, 4 * T : 5 * T] = dk[i * T : (i + 1) * T].astype(bf16)
        ysend[i, 5 * T : 6 * T] = dv[i * T : (i + 1) * T].astype(bf16)


def finish_body(place, yrecv, xt, q_out, k_out, v_out, zs, dq):
    y = place[1]

    def total(lo, hi):
        w = [yrecv[i, lo:hi].astype(f32) for i in range(NY)]
        return (w[0] + w[1]) + (w[2] + w[3])

    dq[...] = (total(0, 4 * T) * SCALE).astype(bf16)
    q_out[...] = dq[pl.ds(pl.multiple_of(y * T, T), T)]
    k_out[...] = (total(4 * T, 5 * T) * SCALE).astype(bf16)
    v_out[...] = total(5 * T, 6 * T).astype(bf16)
    acc = None
    for i in range(NY):
        part = nn(xt[:, i].reshape(NX * NC * 64, T), dq[i * T : (i + 1) * T])
        acc = part if acc is None else acc + part
    zs[...] = acc.astype(bf16).reshape(NZ, 32, H)


def vmem(count):
    return [pl.BlockSpec(memory_space=pltpu.VMEM)] * count


def call(body, name, out_shape, scratch, count):
    return pl.pallas_call(
        body,
        name=name,
        in_specs=[pl.BlockSpec(memory_space=pltpu.SMEM)] + vmem(count),
        out_specs=tuple(vmem(len(out_shape))),
        out_shape=tuple(jax.ShapeDtypeStruct(s, d) for s, d in out_shape),
        scratch_shapes=scratch,
    )


def per_device(q, k, v, g, lse, o, do, x):
    place = jnp.stack([lax.axis_index("z"), lax.axis_index("y")]).astype(jnp.int32)
    pack = call(pack_body, "pack", [((NZ, ZB, H), bf16), ((YB, H), bf16)], [], 7)
    zsend, own = pack(place, q, k, v, g.reshape(1, T), lse.reshape(1, T), o, do)
    recv = lax.all_to_all(zsend, "z", 0, 0, tiled=True)
    grp = lax.all_gather(own, "y", axis=0, tiled=False)
    xt = x.T.reshape(2, NY, 32, T).transpose(1, 0, 2, 3).reshape(NY, 64, T)
    xt = lax.all_to_all(xt, "y", 0, 0, tiled=True)
    xt = lax.all_gather(xt, TP, axis=0, tiled=False)
    block = (NY * T, H)
    attend = call(attend_body, "attend", [((NY, RB, H), bf16)], [pltpu.VMEM(block, f32)] * 3, 2)
    (ysend,) = attend(place, recv, grp)
    yrecv = lax.all_to_all(ysend, "y", 0, 0, tiled=True)
    one = ((T, H), bf16)
    finish = call(finish_body, "finish", [one, one, one, ((NZ, 32, H), bf16)], [pltpu.VMEM(block, bf16)], 2)
    q_grad, k_grad, v_grad, zs = finish(place, yrecv, xt)
    back = lax.all_to_all(zs, "z", 0, 0, tiled=True)
    return q_grad, k_grad, v_grad, jnp.sum(back.astype(f32), axis=0)


def solution(mesh):
    finer = Mesh(mesh.devices.reshape(NZ, NY, NX, NC), ("z", "y", "x", "c"))
    spec = P(SP, TP)
    return jax.shard_map(
        per_device, mesh=finer, in_specs=(spec,) * 8, out_specs=(spec,) * 4, check_vma=False
    )
```

```python
import functools

import jax
import jax.numpy as jnp
from jax import lax
from jax.experimental import pallas as pl
from jax.experimental.pallas import tpu as pltpu
from jax.sharding import Mesh
from jax.sharding import PartitionSpec as P

SP = ("z", "y")
TP = ("x", "c")
NZ, NY, NX, NC = 16, 4, 4, 2
T = 128
H = 128
SCALE = H**-0.5
ZB = 2 * T + 8
ST = 4 * T
XB = ST + 16
YB = XB + 2 * T
RB = 4 * T + 2 * T
f32 = jnp.float32
bf16 = jnp.bfloat16


def nt(a, b):
    return lax.dot_general(a, b, (((1,), (1,)), ((), ())), preferred_element_type=f32)


def nn(a, b):
    return lax.dot_general(a, b, (((1,), (0,)), ((), ())), preferred_element_type=f32)


def three(x):
    hi = x.astype(bf16)
    rest = x - hi.astype(f32)
    mid = rest.astype(bf16)
    low = (rest - mid.astype(f32)).astype(bf16)
    return [hi, mid, low]


def pack_body(place, q, k, v, g, lse, o, do, x, zsend, own):
    z = place[0]
    terms = o[...].astype(f32) * do[...].astype(f32)
    r = jnp.sum(terms.T, axis=0, keepdims=True)
    gate = g[...]
    a = gate - lse[...]
    zero = jnp.zeros((1, T), bf16)
    q_stats = three(a) + three(r)
    k_stats = three(gate)
    q_rows = jnp.concatenate(q_stats + [zero, zero], axis=0)
    k_rows = jnp.concatenate(k_stats + [zero] * 5, axis=0)
    own[0:T] = q[...]
    own[T : 2 * T] = do[...]
    own[2 * T : 3 * T] = k[...]
    own[3 * T : 4 * T] = v[...]
    own[ST:XB] = jnp.concatenate(q_stats + k_stats + [zero] * 7, axis=0)
    own[XB:YB] = x[...].T

    def one(j, carry):
        @pl.when(j > z)
        def _():
            zsend[j, 0:T] = k[...]
            zsend[j, T : 2 * T] = v[...]
            zsend[j, 2 * T : ZB] = k_rows

        @pl.when(j <= z)
        def _():
            zsend[j, 0:T] = q[...]
            zsend[j, T : 2 * T] = do[...]
            zsend[j, 2 * T : ZB] = q_rows

        return carry

    lax.fori_loop(0, NZ, one, 0)


def joined(rows):
    w = rows.astype(f32)
    return w[0:1] + w[1:2] + w[2:3]


def upright(row):
    i = lax.broadcasted_iota(jnp.int32, (T, T), 0)
    j = lax.broadcasted_iota(jnp.int32, (T, T), 1)
    return jnp.sum(jnp.where(i == j, row, 0.0), axis=1, keepdims=True)


def attend_body(place, recv, grp, ysend, dq, dk, dv):
    z = place[0]
    y = place[1]
    qg = jnp.concatenate([grp[i, 0:T] for i in range(NY)], axis=0)
    dog = jnp.concatenate([grp[i, T : 2 * T] for i in range(NY)], axis=0)
    kg = jnp.concatenate([grp[i, 2 * T : 3 * T] for i in range(NY)], axis=0)
    vg = jnp.concatenate([grp[i, 3 * T : 4 * T] for i in range(NY)], axis=0)
    stats = [grp[i, ST:XB] for i in range(NY)]
    a_col = jnp.concatenate([upright(joined(s[0:3])) for s in stats], axis=0)
    r_col = jnp.concatenate([upright(joined(s[3:6])) for s in stats], axis=0)
    g_col = jnp.concatenate([upright(joined(s[6:9])) for s in stats], axis=0)

    def query_part(k, v, g_row, mask):
        s = nt(qg, k) * SCALE + (a_col - g_row)
        if mask is not None:
            s = jnp.where(mask, s, -jnp.inf)
        w = jnp.exp(s)
        sl = (w * (nt(dog, v) - r_col)).astype(bf16)
        return nn(sl, k)

    def key_part(q, do, a_row, r_row, mask):
        s = nt(kg, q) * SCALE + (a_row - g_col)
        if mask is not None:
            s = jnp.where(mask, s, -jnp.inf)
        w = jnp.exp(s)
        sl = (w * (nt(vg, do) - r_row)).astype(bf16)
        return nn(sl, q), nn(w.astype(bf16), do)

    big = lax.broadcasted_iota(jnp.int32, (NY * T, T), 0)
    small = lax.broadcasted_iota(jnp.int32, (NY * T, T), 1) + y * T
    own_stats = grp[y, ST:XB]
    dq[...] = query_part(grp[y, 2 * T : 3 * T], grp[y, 3 * T : 4 * T], joined(own_stats[6:9]), small <= big)
    first = key_part(
        grp[y, 0:T], grp[y, T : 2 * T], joined(own_stats[0:3]), joined(own_stats[3:6]), big <= small
    )
    dk[...] = first[0]
    dv[...] = first[1]

    def below(j, carry):
        dq[...] += query_part(recv[j, 0:T], recv[j, T : 2 * T], joined(recv[j, 2 * T : ZB][0:3]), None)
        return carry

    def above(j, carry):
        rows = recv[j, 2 * T : ZB]
        more = key_part(recv[j, 0:T], recv[j, T : 2 * T], joined(rows[0:3]), joined(rows[3:6]), None)
        dk[...] += more[0]
        dv[...] += more[1]
        return carry

    lax.fori_loop(0, z, below, 0)
    lax.fori_loop(z + 1, NZ, above, 0)
    sums = dq[...].astype(bf16)
    for i in range(NY):
        ysend[i, 0 : 4 * T] = sums
        ysend[i, 4 * T : 5 * T] = dk[i * T : (i + 1) * T].astype(bf16)
        ysend[i, 5 * T : 6 * T] = dv[i * T : (i + 1) * T].astype(bf16)


def finish_body(place, yrecv, xt, q_out, k_out, v_out, zs, dq):
    y = place[1]

    def total(lo, hi):
        w = [yrecv[i, lo:hi].astype(f32) for i in range(NY)]
        return (w[0] + w[1]) + (w[2] + w[3])

    dq[...] = (total(0, 4 * T) * SCALE).astype(bf16)
    q_out[...] = dq[pl.ds(pl.multiple_of(y * T, T), T)]
    k_out[...] = (total(4 * T, 5 * T) * SCALE).astype(bf16)
    v_out[...] = total(5 * T, 6 * T).astype(bf16)
    acc = None
    for i in range(NY):
        part = nn(xt[:, i].reshape(NX * NC * 64, T), dq[i * T : (i + 1) * T])
        acc = part if acc is None else acc + part
    zs[...] = acc.astype(bf16).reshape(NZ, 32, H)


def vmem(count):
    return [pl.BlockSpec(memory_space=pltpu.VMEM)] * count


def call(body, name, out_shape, scratch, count):
    return pl.pallas_call(
        body,
        name=name,
        in_specs=[pl.BlockSpec(memory_space=pltpu.SMEM)] + vmem(count),
        out_specs=tuple(vmem(len(out_shape))),
        out_shape=tuple(jax.ShapeDtypeStruct(s, d) for s, d in out_shape),
        scratch_shapes=scratch,
    )


def per_device(q, k, v, g, lse, o, do, x):
    place = jnp.stack([lax.axis_index("z"), lax.axis_index("y")]).astype(jnp.int32)
    pack = call(pack_body, "pack", [((NZ, ZB, H), bf16), ((YB, H), bf16)], [], 8)
    zsend, own = pack(place, q, k, v, g.reshape(1, T), lse.reshape(1, T), o, do, x)
    recv = lax.all_to_all(zsend, "z", 0, 0, tiled=True)
    grp = lax.all_gather(own, "y", axis=0, tiled=False)
    y = lax.axis_index("y")
    part = [lax.dynamic_slice_in_dim(grp, XB + half * T + y * 32, 32, 1) for half in range(2)]
    xt = lax.all_gather(jnp.concatenate(part, axis=1), TP, axis=0, tiled=False)
    recv, xt = lax.optimization_barrier((recv, xt))
    block = (NY * T, H)
    attend = call(attend_body, "attend", [((NY, RB, H), bf16)], [pltpu.VMEM(block, f32)] * 3, 2)
    (ysend,) = attend(place, recv, grp)
    yrecv = lax.all_to_all(ysend, "y", 0, 0, tiled=True)
    one = ((T, H), bf16)
    finish = call(finish_body, "finish", [one, one, one, ((NZ, 32, H), bf16)], [pltpu.VMEM(block, bf16)], 2)
    q_grad, k_grad, v_grad, zs = finish(place, yrecv, xt)
    back = lax.all_to_all(zs, "z", 0, 0, tiled=True)
    return q_grad, k_grad, v_grad, jnp.sum(back.astype(f32), axis=0)


def solution(mesh):
    finer = Mesh(mesh.devices.reshape(NZ, NY, NX, NC), ("z", "y", "x", "c"))
    spec = P(SP, TP)
    return jax.shard_map(
        per_device, mesh=finer, in_specs=(spec,) * 8, out_specs=(spec,) * 4, check_vma=False
    )
```

```python
import jax
import jax.numpy as jnp
from jax import lax
from jax.experimental import pallas as pl
from jax.experimental.pallas import tpu as pltpu
from jax.sharding import Mesh
from jax.sharding import PartitionSpec as P

SP = ("zp", "zl", "y")
TP = ("x", "c")
NZ, NP, NY, NX, NC = 16, 8, 4, 4, 2
T = 128
H = 128
SCALE = H**-0.5
ZB = 2 * T + 8
ST = 4 * T
XB = ST + 16
YB = XB + 2 * T
RB = 4 * T + 2 * T
f32 = jnp.float32
bf16 = jnp.bfloat16


def nt(a, b):
    return lax.dot_general(a, b, (((1,), (1,)), ((), ())), preferred_element_type=f32)


def nn(a, b):
    return lax.dot_general(a, b, (((1,), (0,)), ((), ())), preferred_element_type=f32)


def three(x):
    hi = x.astype(bf16)
    rest = x - hi.astype(f32)
    mid = rest.astype(bf16)
    low = (rest - mid.astype(f32)).astype(bf16)
    return [hi, mid, low]


def pack_body(place, q, k, v, g, lse, o, do, x, zsend, own):
    zp = place[0]
    zl = place[1]
    terms = o[...].astype(f32) * do[...].astype(f32)
    r = jnp.sum(terms.T, axis=0, keepdims=True)
    gate = g[...]
    a = gate - lse[...]
    zero = jnp.zeros((1, T), bf16)
    q_stats = three(a) + three(r)
    k_stats = three(gate)
    q_rows = jnp.concatenate(q_stats + [zero, zero], axis=0)
    k_rows = jnp.concatenate(k_stats + [zero] * 5, axis=0)
    own[0:T] = q[...]
    own[T : 2 * T] = do[...]
    own[2 * T : 3 * T] = k[...]
    own[3 * T : 4 * T] = v[...]
    own[ST:XB] = jnp.concatenate(q_stats + k_stats + [zero] * 7, axis=0)
    own[XB:YB] = x[...].T

    def one(j, carry):
        up = j + 1 > zp + zl

        @pl.when(up)
        def _():
            zsend[j, 0:T] = k[...]
            zsend[j, T : 2 * T] = v[...]
            zsend[j, 2 * T : ZB] = k_rows

        @pl.when(jnp.logical_not(up))
        def _():
            zsend[j, 0:T] = q[...]
            zsend[j, T : 2 * T] = do[...]
            zsend[j, 2 * T : ZB] = q_rows

        return carry

    lax.fori_loop(0, NP, one, 0)


def joined(rows):
    w = rows.astype(f32)
    return w[0:1] + w[1:2] + w[2:3]


def upright(row):
    i = lax.broadcasted_iota(jnp.int32, (T, T), 0)
    j = lax.broadcasted_iota(jnp.int32, (T, T), 1)
    return jnp.sum(jnp.where(i == j, row, 0.0), axis=1, keepdims=True)


def tall(grp, at):
    return jnp.concatenate([grp[i, at : at + T] for i in range(NY)], axis=0)


def tall_stat(grp, at):
    return jnp.concatenate([upright(joined(grp[i, ST:XB][at : at + 3])) for i in range(NY)], axis=0)


def parts_of(grp):
    qg, dog, kg, vg = (tall(grp, i * T) for i in range(4))
    a_col, r_col, g_col = (tall_stat(grp, 3 * i) for i in range(3))

    def query_part(k, v, g_row, mask=None):
        s = nt(qg, k) * SCALE + (a_col - g_row)
        if mask is not None:
            s = jnp.where(mask, s, -jnp.inf)
        w = jnp.exp(s)
        sl = (w * (nt(dog, v) - r_col)).astype(bf16)
        return nn(sl, k)

    def key_part(q, do, a_row, r_row, mask=None):
        s = nt(kg, q) * SCALE + (a_row - g_col)
        if mask is not None:
            s = jnp.where(mask, s, -jnp.inf)
        w = jnp.exp(s)
        sl = (w * (nt(vg, do) - r_row)).astype(bf16)
        return nn(sl, q), nn(w.astype(bf16), do)

    return query_part, key_part


def received(recv, query_part, key_part, below_end, above_start, dq, dk, dv):
    def below(j, carry):
        rows = recv[j, 2 * T : ZB]
        dq[...] += query_part(recv[j, 0:T], recv[j, T : 2 * T], joined(rows[0:3]))
        return carry

    def above(j, carry):
        rows = recv[j, 2 * T : ZB]
        more = key_part(recv[j, 0:T], recv[j, T : 2 * T], joined(rows[0:3]), joined(rows[3:6]))
        dk[...] += more[0]
        dv[...] += more[1]
        return carry

    lax.fori_loop(0, below_end, below, 0)
    lax.fori_loop(above_start, NP, above, 0)


def first_body(place, recv, grp, dq, dk, dv):
    zp = place[0]
    y = place[2]
    query_part, key_part = parts_of(grp)
    big = lax.broadcasted_iota(jnp.int32, (NY * T, T), 0)
    small = lax.broadcasted_iota(jnp.int32, (NY * T, T), 1) + y * T
    st = grp[y, ST:XB]
    dq[...] = query_part(grp[y, 2 * T : 3 * T], grp[y, 3 * T : 4 * T], joined(st[6:9]), small <= big)
    dk[...], dv[...] = key_part(
        grp[y, 0:T], grp[y, T : 2 * T], joined(st[0:3]), joined(st[3:6]), big <= small
    )
    received(recv, query_part, key_part, zp, zp + 1, dq, dk, dv)


def second_body(place, recv, grp, dq0, dk0, dv0, ysend, dq, dk, dv):
    border = place[0] + place[1]
    query_part, key_part = parts_of(grp)
    dq[...] = dq0[...]
    dk[...] = dk0[...]
    dv[...] = dv0[...]
    received(recv, query_part, key_part, border, border, dq, dk, dv)
    sums = dq[...].astype(bf16)
    for i in range(NY):
        ysend[i, 0 : 4 * T] = sums
        ysend[i, 4 * T : 5 * T] = dk[i * T : (i + 1) * T].astype(bf16)
        ysend[i, 5 * T : 6 * T] = dv[i * T : (i + 1) * T].astype(bf16)


def finish_body(place, yrecv, xt, q_out, k_out, v_out, zs, dq):
    y = place[2]

    def total(lo, hi):
        w = [yrecv[i, lo:hi].astype(f32) for i in range(NY)]
        return (w[0] + w[1]) + (w[2] + w[3])

    dq[...] = (total(0, 4 * T) * SCALE).astype(bf16)
    q_out[...] = dq[pl.ds(pl.multiple_of(y * T, T), T)]
    k_out[...] = (total(4 * T, 5 * T) * SCALE).astype(bf16)
    v_out[...] = total(5 * T, 6 * T).astype(bf16)
    acc = None
    for i in range(NY):
        part = nn(xt[:, i].reshape(NX * NC * 64, T), dq[i * T : (i + 1) * T])
        acc = part if acc is None else acc + part
    zs[...] = acc.astype(bf16).reshape(NZ, 32, H)


def vmem(count):
    return [pl.BlockSpec(memory_space=pltpu.VMEM)] * count


def call(body, name, out_shape, scratch, count):
    return pl.pallas_call(
        body,
        name=name,
        in_specs=[pl.BlockSpec(memory_space=pltpu.SMEM)] + vmem(count),
        out_specs=tuple(vmem(len(out_shape))),
        out_shape=tuple(jax.ShapeDtypeStruct(s, d) for s, d in out_shape),
        scratch_shapes=scratch,
    )


def per_device(q, k, v, g, lse, o, do, x):
    y = lax.axis_index("y")
    place = jnp.stack([lax.axis_index("zp"), lax.axis_index("zl"), y]).astype(jnp.int32)
    pack = call(pack_body, "pack", [((NP, ZB, H), bf16), ((YB, H), bf16)], [], 8)
    zsend, own = pack(place, q, k, v, g.reshape(1, T), lse.reshape(1, T), o, do, x)
    recv = lax.all_to_all(zsend, "zp", 0, 0, tiled=True)
    grp = lax.all_gather(own, "y", axis=0, tiled=False)
    part = [lax.dynamic_slice_in_dim(grp, XB + half * T + y * 32, 32, 1) for half in range(2)]
    xt = lax.all_gather(jnp.concatenate(part, axis=1), TP, axis=0, tiled=False)
    recv, xt = lax.optimization_barrier((recv, xt))
    relayed = lax.ppermute(recv, "zl", [(0, 1), (1, 0)])
    block = (NY * T, H)
    first = call(first_body, "first", [(block, f32)] * 3, [], 2)
    sums = first(place, recv, grp)
    second = call(second_body, "second", [((NY, RB, H), bf16)], [pltpu.VMEM(block, f32)] * 3, 5)
    (ysend,) = second(place, relayed, grp, *sums)
    yrecv = lax.all_to_all(ysend, "y", 0, 0, tiled=True)
    one = ((T, H), bf16)
    finish = call(finish_body, "finish", [one, one, one, ((NZ, 32, H), bf16)], [pltpu.VMEM(block, bf16)], 2)
    q_grad, k_grad, v_grad, zs = finish(place, yrecv, xt)
    back = lax.all_to_all(zs, ("zp", "zl"), 0, 0, tiled=True)
    return q_grad, k_grad, v_grad, jnp.sum(back.astype(f32), axis=0)


def solution(mesh):
    finer = Mesh(mesh.devices.reshape(NP, 2, NY, NX, NC), SP + TP)
    spec = P(SP, TP)
    return jax.shard_map(
        per_device, mesh=finer, in_specs=(spec,) * 8, out_specs=(spec,) * 4, check_vma=False
    )
```

```python
import jax
import jax.numpy as jnp
from jax import lax
from jax.experimental import pallas as pl
from jax.experimental.pallas import tpu as pltpu
from jax.sharding import Mesh
from jax.sharding import PartitionSpec as P

SP = ("zp", "zl", "y")
TP = ("x", "c")
NP, NY, NX, NC = 8, 4, 4, 2
T = 128
H = 128
SCALE = H**-0.5
ZB = 2 * T + 8
ST = 4 * T
XB = ST + 16
YB = XB + 2 * T
f32 = jnp.float32
bf16 = jnp.bfloat16


def nt(a, b):
    return lax.dot_general(a, b, (((1,), (1,)), ((), ())), preferred_element_type=f32)


def nn(a, b):
    return lax.dot_general(a, b, (((1,), (0,)), ((), ())), preferred_element_type=f32)


def three(x):
    hi = x.astype(bf16)
    rest = x - hi.astype(f32)
    mid = rest.astype(bf16)
    low = (rest - mid.astype(f32)).astype(bf16)
    return [hi, mid, low]


def pack_body(place, q, k, v, g, lse, o, do, x, zsend, own):
    zp = place[0]
    zl = place[1]
    terms = o[...].astype(f32) * do[...].astype(f32)
    r = jnp.sum(terms.T, axis=0, keepdims=True)
    gate = g[...]
    a = gate - lse[...]
    zero = jnp.zeros((1, T), bf16)
    q_stats = three(a) + three(r)
    k_stats = three(gate)
    q_rows = jnp.concatenate(q_stats + [zero, zero], axis=0)
    k_rows = jnp.concatenate(k_stats + [zero] * 5, axis=0)
    own[0:T] = q[...]
    own[T : 2 * T] = do[...]
    own[2 * T : 3 * T] = k[...]
    own[3 * T : 4 * T] = v[...]
    own[ST:XB] = jnp.concatenate(q_stats + k_stats + [zero] * 7, axis=0)
    own[XB:YB] = x[...].T

    def one(j, carry):
        up = j + 1 > zp + zl

        @pl.when(up)
        def _():
            zsend[j, 0:T] = k[...]
            zsend[j, T : 2 * T] = v[...]
            zsend[j, 2 * T : ZB] = k_rows

        @pl.when(jnp.logical_not(up))
        def _():
            zsend[j, 0:T] = q[...]
            zsend[j, T : 2 * T] = do[...]
            zsend[j, 2 * T : ZB] = q_rows

        return carry

    lax.fori_loop(0, NP, one, 0)


def joined(rows):
    w = rows.astype(f32)
    return w[0:1] + w[1:2] + w[2:3]


def upright(row):
    i = lax.broadcasted_iota(jnp.int32, (T, T), 0)
    j = lax.broadcasted_iota(jnp.int32, (T, T), 1)
    return jnp.sum(jnp.where(i == j, row, 0.0), axis=1, keepdims=True)


def tall(grp, at):
    return jnp.concatenate([grp[i, at : at + T] for i in range(NY)], axis=0)


def tall_stat(grp, at):
    return jnp.concatenate([upright(joined(grp[i, ST:XB][at : at + 3])) for i in range(NY)], axis=0)


def parts_of(grp):
    qg, dog, kg, vg = (tall(grp, i * T) for i in range(4))
    a_col, r_col, g_col = (tall_stat(grp, 3 * i) for i in range(3))

    def query_part(k, v, g_row, mask=None):
        s = nt(qg, k) * SCALE + (a_col - g_row)
        if mask is not None:
            s = jnp.where(mask, s, -jnp.inf)
        w = jnp.exp(s)
        sl = (w * (nt(dog, v) - r_col)).astype(bf16)
        return nn(sl, k)

    def key_part(q, do, a_row, r_row, mask=None):
        s = nt(kg, q) * SCALE + (a_row - g_col)
        if mask is not None:
            s = jnp.where(mask, s, -jnp.inf)
        w = jnp.exp(s)
        sl = (w * (nt(vg, do) - r_row)).astype(bf16)
        return nn(sl, q), nn(w.astype(bf16), do)

    return query_part, key_part


def received(recv, query_part, key_part, below_end, above_start, dq, dk, dv):
    def below(j, carry):
        rows = recv[j, 2 * T : ZB]
        dq[...] += query_part(recv[j, 0:T], recv[j, T : 2 * T], joined(rows[0:3]))
        return carry

    def above(j, carry):
        rows = recv[j, 2 * T : ZB]
        more = key_part(recv[j, 0:T], recv[j, T : 2 * T], joined(rows[0:3]), joined(rows[3:6]))
        dk[...] += more[0]
        dv[...] += more[1]
        return carry

    lax.fori_loop(0, below_end, below, 0)
    lax.fori_loop(above_start, NP, above, 0)


def first_body(place, recv, grp, dq, dk, dv):
    zp = place[0]
    y = place[2]
    query_part, key_part = parts_of(grp)
    big = lax.broadcasted_iota(jnp.int32, (NY * T, T), 0)
    small = lax.broadcasted_iota(jnp.int32, (NY * T, T), 1) + y * T
    st = grp[y, ST:XB]
    dq[...] = query_part(grp[y, 2 * T : 3 * T], grp[y, 3 * T : 4 * T], joined(st[6:9]), small <= big)
    dk[...], dv[...] = key_part(
        grp[y, 0:T], grp[y, T : 2 * T], joined(st[0:3]), joined(st[3:6]), big <= small
    )
    received(recv, query_part, key_part, zp, zp + 1, dq, dk, dv)


def second_body(place, recv, grp, dq0, dk0, dv0, q_sums, *rest):
    kv_sums, (dq, dk, dv) = rest[:NY], rest[NY:]
    border = place[0] + place[1]
    y = place[2]
    query_part, key_part = parts_of(grp)
    dq[...] = dq0[...]
    dk[...] = dk0[...]
    dv[...] = dv0[...]
    received(recv, query_part, key_part, border, border, dq, dk, dv)
    sums = dq[...].astype(bf16)
    for d in range(NY):
        at = pl.ds(pl.multiple_of(((y + d) % NY) * T, T), T)
        q_sums[d] = sums
        kv_sums[d][0:T] = dk[at].astype(bf16)
        kv_sums[d][T : 2 * T] = dv[at].astype(bf16)


def finish_body(place, q_sums, xt, q_out, keep, send, dq, wg):
    zl = place[1]
    y = place[2]
    w = [q_sums[i].astype(f32) for i in range(NY)]
    dq[...] = (((w[0] + w[1]) + (w[2] + w[3])) * SCALE).astype(bf16)
    q_out[...] = dq[pl.ds(pl.multiple_of(y * T, T), T)]
    acc = None
    for i in range(NY):
        part = nn(xt[:, i].reshape(NP * 64, T), dq[i * T : (i + 1) * T])
        acc = part if acc is None else acc + part
    wg[...] = acc.reshape(NP, 2, 32, H)
    keep[...] = wg[:, pl.ds(zl, 1)].reshape(NP, 32, H)
    send[...] = wg[:, pl.ds(1 - zl, 1)].reshape(NP, 32, H).astype(bf16)


def vmem(count):
    return [pl.BlockSpec(memory_space=pltpu.VMEM)] * count


def call(body, out_shape, scratch, count):
    return pl.pallas_call(
        body,
        in_specs=[pl.BlockSpec(memory_space=pltpu.SMEM)] + vmem(count),
        out_specs=tuple(vmem(len(out_shape))),
        out_shape=tuple(jax.ShapeDtypeStruct(s, d) for s, d in out_shape),
        scratch_shapes=scratch,
    )


def per_device(q, k, v, g, lse, o, do, x):
    y = lax.axis_index("y")
    place = jnp.stack([lax.axis_index("zp"), lax.axis_index("zl"), y]).astype(jnp.int32)
    pack = call(pack_body, [((NP, ZB, H), bf16), ((YB, H), bf16)], [], 8)
    zsend, own = pack(place, q, k, v, g.reshape(1, T), lse.reshape(1, T), o, do, x)
    recv = lax.all_to_all(zsend, "zp", 0, 0, tiled=True)
    grp = lax.all_gather(own, "y", axis=0, tiled=False)
    part = [lax.dynamic_slice_in_dim(grp, XB + half * T + y * 32, 32, 1) for half in range(2)]
    xt = lax.all_gather(jnp.concatenate(part, axis=1), TP, axis=0, tiled=False)
    recv, xt = lax.optimization_barrier((recv, xt))
    relayed = lax.ppermute(recv, "zl", [(0, 1), (1, 0)])
    block = (NY * T, H)
    first = call(first_body, [(block, f32)] * 3, [], 2)
    sums = first(place, recv, grp)
    kv_block = ((2 * T, H), bf16)
    second = call(
        second_body, [((NY, NY * T, H), bf16)] + [kv_block] * NY, [pltpu.VMEM(block, f32)] * 3, 5
    )
    q_sums, *kv = second(place, relayed, grp, *sums)
    q_sums = lax.all_to_all(q_sums, "y", 0, 0, tiled=True)
    part = (NP, 32, H)
    finish = call(
        finish_body,
        [((T, H), bf16), (part, f32), (part, bf16)],
        [pltpu.VMEM(block, bf16), pltpu.VMEM((NP, 2, 32, H), f32)],
        2,
    )
    q_grad, keep, send = finish(place, q_sums, xt)
    other = lax.ppermute(send, "zl", [(0, 1), (1, 0)])
    pair = (keep + other.astype(f32)).astype(bf16)
    pair, *kv = lax.optimization_barrier((pair, *kv))
    back = lax.all_to_all(pair, "zp", 0, 0, tiled=True)
    total = kv[0].astype(f32)
    for d in range(1, NY):
        turn = [(i, (i + d) % NY) for i in range(NY)]
        turned = lax.ppermute(kv[d], "y", turn)
        total = total + turned.astype(f32)
    k_grad = (total[0:T] * SCALE).astype(bf16)
    v_grad = total[T : 2 * T].astype(bf16)
    return q_grad, k_grad, v_grad, jnp.sum(back.astype(f32), axis=0)


def solution(mesh):
    finer = Mesh(mesh.devices.reshape(NP, 2, NY, NX, NC), SP + TP)
    spec = P(SP, TP)
    return jax.shard_map(
        per_device, mesh=finer, in_specs=(spec,) * 8, out_specs=(spec,) * 4, check_vma=False
    )
```

```python
import jax
import jax.numpy as jnp
from jax import lax
from jax.experimental import pallas as pl
from jax.experimental.pallas import tpu as pltpu
from jax.sharding import Mesh
from jax.sharding import PartitionSpec as P

SP = ("zp", "zl", "y")
TP = ("x", "c")
NZ, NP, NY, NX, NC = 16, 8, 4, 4, 2
T = 128
H = 128
SCALE = H**-0.5
ZB = 2 * T + 8
ST = 4 * T
XB = ST + 16
YB = XB + 2 * T
f32 = jnp.float32
bf16 = jnp.bfloat16


def nt(a, b):
    return lax.dot_general(a, b, (((1,), (1,)), ((), ())), preferred_element_type=f32)


def nn(a, b):
    return lax.dot_general(a, b, (((1,), (0,)), ((), ())), preferred_element_type=f32)


def three(x):
    hi = x.astype(bf16)
    rest = x - hi.astype(f32)
    mid = rest.astype(bf16)
    low = (rest - mid.astype(f32)).astype(bf16)
    return [hi, mid, low]


def pack_body(place, q, k, v, g, lse, o, do, x, zsend, own):
    zp = place[0]
    zl = place[1]
    terms = o[...].astype(f32) * do[...].astype(f32)
    r = jnp.sum(terms.T, axis=0, keepdims=True)
    gate = g[...]
    a = gate - lse[...]
    zero = jnp.zeros((1, T), bf16)
    q_stats = three(a) + three(r)
    k_stats = three(gate)
    q_rows = jnp.concatenate(q_stats + [zero, zero], axis=0)
    k_rows = jnp.concatenate(k_stats + [zero] * 5, axis=0)
    own[0:T] = q[...]
    own[T : 2 * T] = do[...]
    own[2 * T : 3 * T] = k[...]
    own[3 * T : 4 * T] = v[...]
    own[ST:XB] = jnp.concatenate(q_stats + k_stats + [zero] * 7, axis=0)
    own[XB:YB] = x[...].T

    def one(j, carry):
        up = j + 1 > zp + zl

        @pl.when(up)
        def _():
            zsend[j, 0:T] = k[...]
            zsend[j, T : 2 * T] = v[...]
            zsend[j, 2 * T : ZB] = k_rows

        @pl.when(jnp.logical_not(up))
        def _():
            zsend[j, 0:T] = q[...]
            zsend[j, T : 2 * T] = do[...]
            zsend[j, 2 * T : ZB] = q_rows

        return carry

    lax.fori_loop(0, NP, one, 0)


def joined(rows):
    w = rows.astype(f32)
    return w[0:1] + w[1:2] + w[2:3]


def upright(row):
    i = lax.broadcasted_iota(jnp.int32, (T, T), 0)
    j = lax.broadcasted_iota(jnp.int32, (T, T), 1)
    return jnp.sum(jnp.where(i == j, row, 0.0), axis=1, keepdims=True)


def tall(grp, at):
    return jnp.concatenate([grp[i, at : at + T] for i in range(NY)], axis=0)


def tall_stat(grp, at):
    return jnp.concatenate([upright(joined(grp[i, ST:XB][at : at + 3])) for i in range(NY)], axis=0)


def parts_of(grp):
    qg, dog, kg, vg = (tall(grp, i * T) for i in range(4))
    a_col, r_col, g_col = (tall_stat(grp, 3 * i) for i in range(3))

    def query_part(k, v, g_row, mask=None):
        s = nt(qg, k) * SCALE + (a_col - g_row)
        if mask is not None:
            s = jnp.where(mask, s, -jnp.inf)
        w = jnp.exp(s)
        sl = (w * (nt(dog, v) - r_col)).astype(bf16)
        return nn(sl, k)

    def key_part(q, do, a_row, r_row, mask=None):
        s = nt(kg, q) * SCALE + (a_row - g_col)
        if mask is not None:
            s = jnp.where(mask, s, -jnp.inf)
        w = jnp.exp(s)
        sl = (w * (nt(vg, do) - r_row)).astype(bf16)
        return nn(sl, q), nn(w.astype(bf16), do)

    return query_part, key_part


def received(recv, query_part, key_part, below_end, above_start, dq, dk, dv):
    def block(j, count, at):
        return recv[pl.ds(j, count), at * T : (at + 1) * T].reshape(count * T, H)

    def stat(j, count, at):
        rows = [joined(recv[j + i, 2 * T : ZB][at : at + 3]) for i in range(count)]
        return jnp.concatenate(rows, axis=1)

    def below(j, count):
        dq[...] += query_part(block(j, count, 0), block(j, count, 1), stat(j, count, 0))

    def above(j, count):
        more = key_part(block(j, count, 0), block(j, count, 1), stat(j, count, 0), stat(j, count, 3))
        dk[...] += more[0]
        dv[...] += more[1]

    def over(step, start, end):
        twos = (end - start) // 2

        def two(i, carry):
            step(start + 2 * i, 2)
            return carry

        lax.fori_loop(0, twos, two, 0)

        @pl.when(start + 2 * twos < end)
        def _():
            step(end - 1, 1)

    over(below, 0, below_end)
    over(above, above_start, NP)


def first_body(place, recv, grp, dq, dk, dv):
    zp = place[0]
    y = place[2]
    query_part, key_part = parts_of(grp)
    big = lax.broadcasted_iota(jnp.int32, (NY * T, T), 0)
    small = lax.broadcasted_iota(jnp.int32, (NY * T, T), 1) + y * T
    st = grp[y, ST:XB]
    dq[...] = query_part(grp[y, 2 * T : 3 * T], grp[y, 3 * T : 4 * T], joined(st[6:9]), small <= big)
    dk[...], dv[...] = key_part(
        grp[y, 0:T], grp[y, T : 2 * T], joined(st[0:3]), joined(st[3:6]), big <= small
    )
    received(recv, query_part, key_part, zp, zp + 1, dq, dk, dv)


def second_body(place, recv, grp, dq0, dk0, dv0, ysend, dq, dk, dv):
    border = place[0] + place[1]
    query_part, key_part = parts_of(grp)
    dq[...] = dq0[...]
    dk[...] = dk0[...]
    dv[...] = dv0[...]
    received(recv, query_part, key_part, border, border, dq, dk, dv)
    sums = dq[...].astype(bf16)
    for i in range(NY):
        ysend[i, 0 : 4 * T] = sums
        ysend[i, 4 * T : 5 * T] = dk[i * T : (i + 1) * T].astype(bf16)
        ysend[i, 5 * T : 6 * T] = dv[i * T : (i + 1) * T].astype(bf16)


def finish_body(place, sums, xt, q_out, k_out, v_out, keep, send, dq, wg):
    zl = place[1]
    y = place[2]

    def total(lo, hi):
        w = [sums[i, lo:hi].astype(f32) for i in range(NY)]
        return (w[0] + w[1]) + (w[2] + w[3])

    dq[...] = (total(0, 4 * T) * SCALE).astype(bf16)
    q_out[...] = dq[pl.ds(pl.multiple_of(y * T, T), T)]
    k_out[...] = (total(4 * T, 5 * T) * SCALE).astype(bf16)
    v_out[...] = total(5 * T, 6 * T).astype(bf16)
    acc = None
    for i in range(NY):
        part = nn(xt[:, i].reshape(NP * 64, T), dq[i * T : (i + 1) * T])
        acc = part if acc is None else acc + part
    wg[...] = acc.reshape(NP, 2, 32, H)
    keep[...] = wg[:, pl.ds(zl, 1)].reshape(NP, 32, H)
    send[...] = wg[:, pl.ds(1 - zl, 1)].reshape(NP, 32, H).astype(bf16)


def vmem(count):
    return [pl.BlockSpec(memory_space=pltpu.VMEM)] * count


def call(body, name, out_shape, scratch, count):
    return pl.pallas_call(
        body,
        name=name,
        in_specs=[pl.BlockSpec(memory_space=pltpu.SMEM)] + vmem(count),
        out_specs=tuple(vmem(len(out_shape))),
        out_shape=tuple(jax.ShapeDtypeStruct(s, d) for s, d in out_shape),
        scratch_shapes=scratch,
    )


def per_device(q, k, v, g, lse, o, do, x):
    y = lax.axis_index("y")
    place = jnp.stack([lax.axis_index("zp"), lax.axis_index("zl"), y]).astype(jnp.int32)
    pack = call(pack_body, "pack", [((NP, ZB, H), bf16), ((YB, H), bf16)], [], 8)
    zsend, own = pack(place, q, k, v, g.reshape(1, T), lse.reshape(1, T), o, do, x)
    recv = lax.all_to_all(zsend, "zp", 0, 0, tiled=True)
    grp = lax.all_gather(own, "y", axis=0, tiled=False)
    part = [lax.dynamic_slice_in_dim(grp, XB + half * T + y * 32, 32, 1) for half in range(2)]
    xt = lax.all_gather(jnp.concatenate(part, axis=1), TP, axis=0, tiled=False)
    recv, xt = lax.optimization_barrier((recv, xt))
    relayed = lax.ppermute(recv, "zl", [(0, 1), (1, 0)])
    block = (NY * T, H)
    first = call(first_body, "first", [(block, f32)] * 3, [], 2)
    sums = first(place, recv, grp)
    second = call(second_body, "second", [((NY, 6 * T, H), bf16)], [pltpu.VMEM(block, f32)] * 3, 5)
    (ysend,) = second(place, relayed, grp, *sums)
    sums = lax.all_to_all(ysend, "y", 0, 0, tiled=True)
    one, part = ((T, H), bf16), (NP, 32, H)
    finish = call(
        finish_body,
        "finish",
        [one, one, one, (part, f32), (part, bf16)],
        [pltpu.VMEM(block, bf16), pltpu.VMEM((NP, 2, 32, H), f32)],
        2,
    )
    q_grad, k_grad, v_grad, keep, send = finish(place, sums, xt)
    other = lax.ppermute(send, "zl", [(0, 1), (1, 0)])
    pair = (keep + other.astype(f32)).astype(bf16)
    back = lax.all_to_all(pair, "zp", 0, 0, tiled=True)
    return q_grad, k_grad, v_grad, jnp.sum(back.astype(f32), axis=0)


def solution(mesh):
    finer = Mesh(mesh.devices.reshape(NP, 2, NY, NX, NC), SP + TP)
    spec = P(SP, TP)
    return jax.shard_map(
        per_device, mesh=finer, in_specs=(spec,) * 8, out_specs=(spec,) * 4, check_vma=False
    )
```

```python
import jax
import jax.numpy as jnp
from jax import lax
from jax.experimental import pallas as pl
from jax.experimental.pallas import tpu as pltpu
from jax.sharding import Mesh
from jax.sharding import PartitionSpec as P

SP = ("zp", "zl", "y")
TP = ("x", "c")
NZ, NP, NY, NX, NC = 16, 8, 4, 4, 2
T = 128
H = 128
SCALE = H**-0.5
ZB = 2 * T + 8
ST = 4 * T
XB = ST + 16
YB = XB + 2 * T
f32 = jnp.float32
bf16 = jnp.bfloat16


def nt(a, b):
    return lax.dot_general(a, b, (((1,), (1,)), ((), ())), preferred_element_type=f32)


def nn(a, b):
    return lax.dot_general(a, b, (((1,), (0,)), ((), ())), preferred_element_type=f32)


def three(x):
    hi = x.astype(bf16)
    rest = x - hi.astype(f32)
    mid = rest.astype(bf16)
    low = (rest - mid.astype(f32)).astype(bf16)
    return [hi, mid, low]


def pack_body(place, q, k, v, g, lse, o, do, x, zsend, own):
    zp = place[0]
    zl = place[1]
    terms = o[...].astype(f32) * do[...].astype(f32)
    r = jnp.sum(terms.T, axis=0, keepdims=True)
    gate = g[...]
    a = gate - lse[...]
    zero = jnp.zeros((1, T), bf16)
    q_stats = three(a) + three(r)
    k_stats = three(gate)
    q_rows = jnp.concatenate(q_stats + [zero, zero], axis=0)
    k_rows = jnp.concatenate(k_stats + [zero] * 5, axis=0)
    own[0:T] = q[...]
    own[T : 2 * T] = do[...]
    own[2 * T : 3 * T] = k[...]
    own[3 * T : 4 * T] = v[...]
    own[ST:XB] = jnp.concatenate(q_stats + k_stats + [zero] * 7, axis=0)
    own[XB:YB] = x[...].T

    def one(j, carry):
        up = j + 1 > zp + zl

        @pl.when(up)
        def _():
            zsend[j, 0:T] = k[...]
            zsend[j, T : 2 * T] = v[...]
            zsend[j, 2 * T : ZB] = k_rows

        @pl.when(jnp.logical_not(up))
        def _():
            zsend[j, 0:T] = q[...]
            zsend[j, T : 2 * T] = do[...]
            zsend[j, 2 * T : ZB] = q_rows

        return carry

    lax.fori_loop(0, NP, one, 0)


def joined(rows):
    w = rows.astype(f32)
    return w[0:1] + w[1:2] + w[2:3]


def upright(row):
    i = lax.broadcasted_iota(jnp.int32, (T, T), 0)
    j = lax.broadcasted_iota(jnp.int32, (T, T), 1)
    return jnp.sum(jnp.where(i == j, row, 0.0), axis=1, keepdims=True)


def tall(grp, at):
    return jnp.concatenate([grp[i, at : at + T] for i in range(NY)], axis=0)


def tall_stat(grp, at):
    return jnp.concatenate([upright(joined(grp[i, ST:XB][at : at + 3])) for i in range(NY)], axis=0)


def parts_of(grp):
    qg, dog, kg, vg = (tall(grp, i * T) for i in range(4))
    a_col, r_col, g_col = (tall_stat(grp, 3 * i) for i in range(3))

    def query_part(k, v, g_row, mask=None):
        s = nt(qg, k) * SCALE + (a_col - g_row)
        if mask is not None:
            s = jnp.where(mask, s, -jnp.inf)
        w = jnp.exp(s)
        sl = (w * (nt(dog, v) - r_col)).astype(bf16)
        return nn(sl, k)

    def key_part(q, do, a_row, r_row, mask=None):
        s = nt(kg, q) * SCALE + (a_row - g_col)
        if mask is not None:
            s = jnp.where(mask, s, -jnp.inf)
        w = jnp.exp(s)
        sl = (w * (nt(vg, do) - r_row)).astype(bf16)
        return nn(sl, q), nn(w.astype(bf16), do)

    return query_part, key_part


def received(recv, query_part, key_part, below_end, above_start, dq, dk, dv):
    def block(j, count, at):
        return recv[pl.ds(j, count), at * T : (at + 1) * T].reshape(count * T, H)

    def stat(j, count, at):
        rows = [joined(recv[j + i, 2 * T : ZB][at : at + 3]) for i in range(count)]
        return jnp.concatenate(rows, axis=1)

    def below(j, count):
        dq[...] += query_part(block(j, count, 0), block(j, count, 1), stat(j, count, 0))

    def above(j, count):
        more = key_part(block(j, count, 0), block(j, count, 1), stat(j, count, 0), stat(j, count, 3))
        dk[...] += more[0]
        dv[...] += more[1]

    def over(step, start, end):
        twos = (end - start) // 2

        def two(i, carry):
            step(start + 2 * i, 2)
            return carry

        lax.fori_loop(0, twos, two, 0)

        @pl.when(start + 2 * twos < end)
        def _():
            step(end - 1, 1)

    over(below, 0, below_end)
    over(above, above_start, NP)


def first_body(place, recv, grp, dq, dk, dv):
    zp = place[0]
    y = place[2]
    query_part, key_part = parts_of(grp)
    big = lax.broadcasted_iota(jnp.int32, (NY * T, T), 0)
    small = lax.broadcasted_iota(jnp.int32, (NY * T, T), 1) + y * T
    st = grp[y, ST:XB]
    dq[...] = query_part(grp[y, 2 * T : 3 * T], grp[y, 3 * T : 4 * T], joined(st[6:9]), small <= big)
    dk[...], dv[...] = key_part(
        grp[y, 0:T], grp[y, T : 2 * T], joined(st[0:3]), joined(st[3:6]), big <= small
    )
    received(recv, query_part, key_part, zp, zp + 1, dq, dk, dv)


def second_body(place, recv, grp, dq0, dk0, dv0, q_sums, *rest):
    kv_sums, (dq, dk, dv) = rest[:NY], rest[NY:]
    border = place[0] + place[1]
    y = place[2]
    query_part, key_part = parts_of(grp)
    dq[...] = dq0[...]
    dk[...] = dk0[...]
    dv[...] = dv0[...]
    received(recv, query_part, key_part, border, border, dq, dk, dv)
    sums = dq[...].astype(bf16)
    for d in range(NY):
        at = pl.ds(pl.multiple_of(((y + d) % NY) * T, T), T)
        q_sums[d] = sums
        kv_sums[d][0:T] = dk[at].astype(bf16)
        kv_sums[d][T : 2 * T] = dv[at].astype(bf16)


def finish_body(place, sums, *rest):
    xt, (q_out, zs, dq) = rest[:NX], rest[NX:]
    y = place[2]
    x = place[3]
    w = [sums[i].astype(f32) for i in range(NY)]
    dq[...] = (((w[0] + w[1]) + (w[2] + w[3])) * SCALE).astype(bf16)
    q_out[...] = dq[pl.ds(pl.multiple_of(y * T, T), T)]
    for d in range(NX):
        acc = None
        for i in range(NY):
            part = nn(xt[d][:, i].reshape(NC * 64, T), dq[i * T : (i + 1) * T])
            acc = part if acc is None else acc + part
        zs[pl.ds(((x - d) % NX) * 4, 4)] = acc.astype(bf16).reshape(4, 32, H)


def vmem(count):
    return [pl.BlockSpec(memory_space=pltpu.VMEM)] * count


def call(body, out_shape, scratch, count):
    return pl.pallas_call(
        body,
        in_specs=[pl.BlockSpec(memory_space=pltpu.SMEM)] + vmem(count),
        out_specs=tuple(vmem(len(out_shape))),
        out_shape=tuple(jax.ShapeDtypeStruct(s, d) for s, d in out_shape),
        scratch_shapes=scratch,
    )


def per_device(q, k, v, g, lse, o, do, x):
    y = lax.axis_index("y")
    place = [lax.axis_index("zp"), lax.axis_index("zl"), y, lax.axis_index("x")]
    place = jnp.stack(place).astype(jnp.int32)
    pack = call(pack_body, [((NP, ZB, H), bf16), ((YB, H), bf16)], [], 8)
    zsend, own = pack(place, q, k, v, g.reshape(1, T), lse.reshape(1, T), o, do, x)
    recv = lax.all_to_all(zsend, "zp", 0, 0, tiled=True)
    grp = lax.all_gather(own, "y", axis=0, tiled=False)
    part = [lax.dynamic_slice_in_dim(grp, XB + half * T + y * 32, 32, 1) for half in range(2)]
    xt = lax.all_gather(jnp.concatenate(part, axis=1), "c", axis=0, tiled=False)
    recv, xt = lax.optimization_barrier((recv, xt))
    xts = [xt]
    relayed = lax.ppermute(recv, "zl", [(0, 1), (1, 0)])
    for d in range(1, NX):
        xts.append(lax.ppermute(xt, "x", [(i, (i + d) % NX) for i in range(NX)]))
    block = (NY * T, H)
    sums = call(first_body, [(block, f32)] * 3, [], 2)(place, recv, grp)
    second = call(
        second_body,
        [((NY, NY * T, H), bf16)] + [((2 * T, H), bf16)] * NY,
        [pltpu.VMEM(block, f32)] * 3,
        5,
    )
    q_sums, *kv = second(place, relayed, grp, *sums)
    q_sums = lax.all_to_all(q_sums, "y", 0, 0, tiled=True)
    outs = [((T, H), bf16), ((NZ, 32, H), bf16)]
    finish = call(finish_body, outs, [pltpu.VMEM(block, bf16)], 1 + NX)
    q_grad, zs = finish(place, q_sums, *xts)
    zs, *kv = lax.optimization_barrier((zs, *kv))
    back = lax.all_to_all(zs, ("zp", "zl"), 0, 0, tiled=True)
    total = kv[0].astype(f32)
    for d in range(1, NY):
        turned = lax.ppermute(kv[d], "y", [(i, (i + d) % NY) for i in range(NY)])
        total = total + turned.astype(f32)
    k_grad = (total[0:T] * SCALE).astype(bf16)
    v_grad = total[T : 2 * T].astype(bf16)
    return q_grad, k_grad, v_grad, jnp.sum(back.astype(f32), axis=0)


def solution(mesh):
    finer = Mesh(mesh.devices.reshape(NP, 2, NY, NX, NC), SP + TP)
    spec = P(SP, TP)
    return jax.shard_map(
        per_device, mesh=finer, in_specs=(spec,) * 8, out_specs=(spec,) * 4, check_vma=False
    )
```

```python
import functools

import jax
import jax.numpy as jnp
from jax import lax
from jax.experimental import pallas as pl
from jax.experimental.pallas import tpu as pltpu
from jax.sharding import Mesh
from jax.sharding import PartitionSpec as P

SP = ("zp", "zl", "y")
TP = ("x", "c")
NZ, NP, NY, NX, NC = 16, 8, 4, 4, 2
CUT = 5
T = 128
H = 128
SCALE = H**-0.5
ZB = 2 * T + 8
ST = 4 * T
XB = ST + 16
YB = XB + 2 * T
f32 = jnp.float32
bf16 = jnp.bfloat16


def nt(a, b):
    return lax.dot_general(a, b, (((1,), (1,)), ((), ())), preferred_element_type=f32)


def nn(a, b):
    return lax.dot_general(a, b, (((1,), (0,)), ((), ())), preferred_element_type=f32)


def three(x):
    hi = x.astype(bf16)
    rest = x - hi.astype(f32)
    mid = rest.astype(bf16)
    low = (rest - mid.astype(f32)).astype(bf16)
    return [hi, mid, low]


def pack_body(q, k, v, g, lse, o, do, x, zsend, own):
    zp, zl, _, _ = position()
    terms = o[...].astype(f32) * do[...].astype(f32)
    r = jnp.sum(terms.T, axis=0, keepdims=True)
    gate = g[...]
    a = gate - lse[...]
    zero = jnp.zeros((1, T), bf16)
    q_stats = three(a) + three(r)
    k_stats = three(gate)
    q_rows = jnp.concatenate(q_stats + [zero, zero], axis=0)
    k_rows = jnp.concatenate(k_stats + [zero] * 5, axis=0)
    own[0:T] = q[...]
    own[T : 2 * T] = do[...]
    own[2 * T : 3 * T] = k[...]
    own[3 * T : 4 * T] = v[...]
    own[ST:XB] = jnp.concatenate(q_stats + k_stats + [zero] * 7, axis=0)
    own[XB:YB] = x[...].T

    def one(j, carry):
        up = j + 1 > zp + zl

        @pl.when(up)
        def _():
            zsend[j, 0:T] = k[...]
            zsend[j, T : 2 * T] = v[...]
            zsend[j, 2 * T : ZB] = k_rows

        @pl.when(jnp.logical_not(up))
        def _():
            zsend[j, 0:T] = q[...]
            zsend[j, T : 2 * T] = do[...]
            zsend[j, 2 * T : ZB] = q_rows

        return carry

    lax.fori_loop(0, NP, one, 0)


def joined(rows):
    w = rows.astype(f32)
    return w[0:1] + w[1:2] + w[2:3]


def upright(row):
    i = lax.broadcasted_iota(jnp.int32, (T, T), 0)
    j = lax.broadcasted_iota(jnp.int32, (T, T), 1)
    return jnp.sum(jnp.where(i == j, row, 0.0), axis=1, keepdims=True)


def tall(grp, at):
    return jnp.concatenate([grp[i, at : at + T] for i in range(NY)], axis=0)


def tall_stat(grp, at):
    return jnp.concatenate([upright(joined(grp[i, ST:XB][at : at + 3])) for i in range(NY)], axis=0)


def parts_of(grp):
    qg, dog, kg, vg = (tall(grp, i * T) for i in range(4))
    a_col, r_col, g_col = (tall_stat(grp, 3 * i) for i in range(3))

    def query_part(k, v, g_row, mask=None):
        s = nt(qg, k) * SCALE + (a_col - g_row)
        if mask is not None:
            s = jnp.where(mask, s, -jnp.inf)
        w = jnp.exp(s)
        sl = (w * (nt(dog, v) - r_col)).astype(bf16)
        return nn(sl, k)

    def key_part(q, do, a_row, r_row, mask=None):
        s = nt(kg, q) * SCALE + (a_row - g_col)
        if mask is not None:
            s = jnp.where(mask, s, -jnp.inf)
        w = jnp.exp(s)
        sl = (w * (nt(vg, do) - r_row)).astype(bf16)
        return nn(sl, q), nn(w.astype(bf16), do)

    return query_part, key_part


def received(recv, query_part, key_part, below_end, above_start, end, dq, dk, dv):
    def block(j, count, at):
        return recv[pl.ds(j, count), at * T : (at + 1) * T].reshape(count * T, H)

    def stat(j, count, at):
        rows = [joined(recv[j + i, 2 * T : ZB][at : at + 3]) for i in range(count)]
        return jnp.concatenate(rows, axis=1)

    def below(j, count):
        dq[...] += query_part(block(j, count, 0), block(j, count, 1), stat(j, count, 0))

    def above(j, count):
        more = key_part(block(j, count, 0), block(j, count, 1), stat(j, count, 0), stat(j, count, 3))
        dk[...] += more[0]
        dv[...] += more[1]

    def over(step, start, end):
        twos = (end - start) // 2

        def two(i, carry):
            step(start + 2 * i, 2)
            return carry

        lax.fori_loop(0, twos, two, 0)

        @pl.when(start + 2 * twos < end)
        def _():
            step(end - 1, 1)

    over(below, 0, below_end)
    over(above, above_start, end)


def first_body(recv, grp, dq, dk, dv):
    zp, _, y, _ = position()
    query_part, key_part = parts_of(grp)
    big = lax.broadcasted_iota(jnp.int32, (NY * T, T), 0)
    small = lax.broadcasted_iota(jnp.int32, (NY * T, T), 1) + y * T
    st = grp[y, ST:XB]
    dq[...] = query_part(grp[y, 2 * T : 3 * T], grp[y, 3 * T : 4 * T], joined(st[6:9]), small <= big)
    dk[...], dv[...] = key_part(
        grp[y, 0:T], grp[y, T : 2 * T], joined(st[0:3]), joined(st[3:6]), big <= small
    )
    received(recv, query_part, key_part, zp, zp + 1, NP, dq, dk, dv)


def more_body(low, recv, grp, dq0, dk0, dv0, dq, dk, dv):
    size = recv.shape[0]
    zp, zl, _, _ = position()
    border = jnp.clip(zp + zl - low, 0, size)
    query_part, key_part = parts_of(grp)
    dq[...] = dq0[...]
    dk[...] = dk0[...]
    dv[...] = dv0[...]
    received(recv, query_part, key_part, border, border, size, dq, dk, dv)


def last_body(recv, grp, dq0, dk0, dv0, q_sums, *rest):
    kv_sums, (dq, dk, dv) = rest[:NY], rest[NY:]
    y = position()[2]
    more_body(CUT, recv, grp, dq0, dk0, dv0, dq, dk, dv)
    sums = dq[...].astype(bf16)
    for d in range(NY):
        at = pl.ds(pl.multiple_of(((y + d) % NY) * T, T), T)
        q_sums[d] = sums
        kv_sums[d][0:T] = dk[at].astype(bf16)
        kv_sums[d][T : 2 * T] = dv[at].astype(bf16)


def finish_body(sums, *rest):
    xt, (q_out, zs, dq) = rest[:NX], rest[NX:]
    _, _, y, x = position()
    w = [sums[i].astype(f32) for i in range(NY)]
    dq[...] = (((w[0] + w[1]) + (w[2] + w[3])) * SCALE).astype(bf16)
    q_out[...] = dq[pl.ds(pl.multiple_of(y * T, T), T)]
    acc = None
    for i in range(0, NY, 2):
        cols = [jnp.concatenate([xt[d][:, i + e].reshape(T, T) for d in range(NX)], axis=0) for e in range(2)]
        part = nn(jnp.concatenate(cols, axis=1), dq[i * T : (i + 2) * T])
        acc = part if acc is None else acc + part
    for d in range(NX):
        zs[pl.ds(((x - d) % NX) * 4, 4)] = acc[d * T : (d + 1) * T].astype(bf16).reshape(4, 32, H)


def vmem(count):
    return [pl.BlockSpec(memory_space=pltpu.VMEM)] * count


def position():
    return [lax.axis_index(n) for n in ("zp", "zl", "y", "x")]


def call(body, out_shape, scratch, count):
    return pl.pallas_call(
        body,
        in_specs=vmem(count),
        out_specs=tuple(vmem(len(out_shape))),
        out_shape=tuple(jax.ShapeDtypeStruct(s, d) for s, d in out_shape),
        scratch_shapes=scratch,
    )


def per_device(q, k, v, g, lse, o, do, x):
    y = lax.axis_index("y")
    pack = call(pack_body, [((NP, ZB, H), bf16), ((YB, H), bf16)], [], 8)
    zsend, own = pack(q, k, v, g.reshape(1, T), lse.reshape(1, T), o, do, x)
    recv = lax.all_to_all(zsend, "zp", 0, 0, tiled=True)
    grp = lax.all_gather(own, "y", axis=0, tiled=False)
    part = [lax.dynamic_slice_in_dim(grp, XB + half * T + y * 32, 32, 1) for half in range(2)]
    xt = lax.all_gather(jnp.concatenate(part, axis=1), "c", axis=0, tiled=False)
    xts = [xt]
    for d in range(1, NX):
        xts.append(lax.ppermute(xt, "x", [(i, (i + d) % NX) for i in range(NX)]))
    recv, *xts[:3] = lax.optimization_barrier((recv, *xts[:3]))
    swap = [(0, 1), (1, 0)]
    relayed = lax.ppermute(recv[:CUT], "zl", swap)
    rest = lax.ppermute(recv[CUT:], "zl", swap)
    block = (NY * T, H)
    sums = call(first_body, [(block, f32)] * 3, [], 2)(recv, grp)
    more = call(functools.partial(more_body, 0), [(block, f32)] * 3, [], 5)
    sums = more(relayed, grp, *sums)
    second = call(
        last_body,
        [((NY, NY * T, H), bf16)] + [((2 * T, H), bf16)] * NY,
        [pltpu.VMEM(block, f32)] * 3,
        5,
    )
    q_sums, *kv = second(rest, grp, *sums)
    q_sums = lax.all_to_all(q_sums, "y", 0, 0, tiled=True)
    outs = [((T, H), bf16), ((NZ, 32, H), bf16)]
    finish = call(finish_body, outs, [pltpu.VMEM(block, bf16)], 1 + NX)
    q_grad, zs = finish(q_sums, *xts)
    zs, *kv = lax.optimization_barrier((zs, *kv))
    back = lax.all_to_all(zs, ("zp", "zl"), 0, 0, tiled=True)
    total = kv[0].astype(f32)
    for d in range(1, NY):
        turned = lax.ppermute(kv[d], "y", [(i, (i + d) % NY) for i in range(NY)])
        total = total + turned.astype(f32)
    k_grad = (total[0:T] * SCALE).astype(bf16)
    v_grad = total[T : 2 * T].astype(bf16)
    return q_grad, k_grad, v_grad, jnp.sum(back.astype(f32), axis=0)


def solution(mesh):
    finer = Mesh(mesh.devices.reshape(NP, 2, NY, NX, NC), SP + TP)
    spec = P(SP, TP)
    return jax.shard_map(
        per_device, mesh=finer, in_specs=(spec,) * 8, out_specs=(spec,) * 4, check_vma=False
    )
```

```python
import jax
import jax.numpy as jnp
from jax import lax
from jax.experimental import pallas as pl
from jax.experimental.pallas import tpu as pltpu
from jax.sharding import Mesh
from jax.sharding import PartitionSpec as P

SP = ("zp", "zl", "y")
TP = ("x", "c")
NZ, NP, NY, NX, NC = 16, 8, 4, 4, 2
GROUPS = [[2 * j + (g ^ (j // 4)) for j in range(NP)] for g in range(2)]
T = 128
H = 128
SCALE = H**-0.5
ZB = 2 * T + 8
ST = 4 * T
XB = ST + 16
YB = XB + 2 * T
f32 = jnp.float32
bf16 = jnp.bfloat16


def nt(a, b):
    return lax.dot_general(a, b, (((1,), (1,)), ((), ())), preferred_element_type=f32)


def nn(a, b):
    return lax.dot_general(a, b, (((1,), (0,)), ((), ())), preferred_element_type=f32)


def three(x):
    hi = x.astype(bf16)
    rest = x - hi.astype(f32)
    mid = rest.astype(bf16)
    low = (rest - mid.astype(f32)).astype(bf16)
    return [hi, mid, low]


def pack_body(q, k, v, g, lse, o, do, x, zsend, own):
    zp, zl, _, _ = position()
    terms = o[...].astype(f32) * do[...].astype(f32)
    r = jnp.sum(terms.T, axis=0, keepdims=True)
    gate = g[...]
    a = gate - lse[...]
    zero = jnp.zeros((1, T), bf16)
    q_stats = three(a) + three(r)
    k_stats = three(gate)
    q_rows = jnp.concatenate(q_stats + [zero, zero], axis=0)
    k_rows = jnp.concatenate(k_stats + [zero] * 5, axis=0)
    own[0:T] = q[...]
    own[T : 2 * T] = do[...]
    own[2 * T : 3 * T] = k[...]
    own[3 * T : 4 * T] = v[...]
    own[ST:XB] = jnp.concatenate(q_stats + k_stats + [zero] * 7, axis=0)
    own[XB:YB] = x[...].T

    def one(j, carry):
        up = j + 1 > zp + zl

        @pl.when(up)
        def _():
            zsend[j, 0:T] = k[...]
            zsend[j, T : 2 * T] = v[...]
            zsend[j, 2 * T : ZB] = k_rows

        @pl.when(jnp.logical_not(up))
        def _():
            zsend[j, 0:T] = q[...]
            zsend[j, T : 2 * T] = do[...]
            zsend[j, 2 * T : ZB] = q_rows

        return carry

    lax.fori_loop(0, NP, one, 0)


def joined(rows):
    w = rows.astype(f32)
    return w[0:1] + w[1:2] + w[2:3]


def upright(row):
    i = lax.broadcasted_iota(jnp.int32, (T, T), 0)
    j = lax.broadcasted_iota(jnp.int32, (T, T), 1)
    return jnp.sum(jnp.where(i == j, row, 0.0), axis=1, keepdims=True)


def tall(grp, at):
    return jnp.concatenate([grp[i, at : at + T] for i in range(NY)], axis=0)


def tall_stat(grp, at):
    return jnp.concatenate([upright(joined(grp[i, ST:XB][at : at + 3])) for i in range(NY)], axis=0)


def parts_of(grp):
    qg, dog, kg, vg = (tall(grp, i * T) for i in range(4))
    a_col, r_col, g_col = (tall_stat(grp, 3 * i) for i in range(3))

    def query_part(k, v, g_row, mask=None):
        s = nt(qg, k) * SCALE + (a_col - g_row)
        if mask is not None:
            s = jnp.where(mask, s, -jnp.inf)
        w = jnp.exp(s)
        sl = (w * (nt(dog, v) - r_col)).astype(bf16)
        return nn(sl, k)

    def key_part(q, do, a_row, r_row, mask=None):
        s = nt(kg, q) * SCALE + (a_row - g_col)
        if mask is not None:
            s = jnp.where(mask, s, -jnp.inf)
        w = jnp.exp(s)
        sl = (w * (nt(vg, do) - r_row)).astype(bf16)
        return nn(sl, q), nn(w.astype(bf16), do)

    return query_part, key_part


def received(recv, query_part, key_part, below_end, above_start, dq, dk, dv):
    def block(j, count, at):
        return recv[pl.ds(j, count), at * T : (at + 1) * T].reshape(count * T, H)

    def stat(j, count, at):
        rows = [joined(recv[j + i, 2 * T : ZB][at : at + 3]) for i in range(count)]
        return jnp.concatenate(rows, axis=1)

    def below(j, count):
        dq[...] += query_part(block(j, count, 0), block(j, count, 1), stat(j, count, 0))

    def above(j, count):
        more = key_part(block(j, count, 0), block(j, count, 1), stat(j, count, 0), stat(j, count, 3))
        dk[...] += more[0]
        dv[...] += more[1]

    def over(step, start, end):
        twos = (end - start) // 2

        def two(i, carry):
            step(start + 2 * i, 2)
            return carry

        lax.fori_loop(0, twos, two, 0)

        @pl.when(start + 2 * twos < end)
        def _():
            step(end - 1, 1)

    over(below, 0, below_end)
    over(above, above_start, NP)


def first_body(recv, grp, dq, dk, dv):
    zp, _, y, _ = position()
    query_part, key_part = parts_of(grp)
    big = lax.broadcasted_iota(jnp.int32, (NY * T, T), 0)
    small = lax.broadcasted_iota(jnp.int32, (NY * T, T), 1) + y * T
    st = grp[y, ST:XB]
    dq[...] = query_part(grp[y, 2 * T : 3 * T], grp[y, 3 * T : 4 * T], joined(st[6:9]), small <= big)
    dk[...], dv[...] = key_part(
        grp[y, 0:T], grp[y, T : 2 * T], joined(st[0:3]), joined(st[3:6]), big <= small
    )
    received(recv, query_part, key_part, zp, zp + 1, dq, dk, dv)


def last_body(recv, grp, dq0, dk0, dv0, q_sums, *rest):
    kv_sums, (dq, dk, dv) = rest[:NY], rest[NY:]
    zp, zl, y, _ = position()
    border = zp + zl
    query_part, key_part = parts_of(grp)
    dq[...] = dq0[...]
    dk[...] = dk0[...]
    dv[...] = dv0[...]
    received(recv, query_part, key_part, border, border, dq, dk, dv)
    sums = dq[...].astype(bf16)
    for d in range(NY):
        at = pl.ds(pl.multiple_of(((y + d) % NY) * T, T), T)
        q_sums[d] = sums
        kv_sums[d][0:T] = dk[at].astype(bf16)
        kv_sums[d][T : 2 * T] = dv[at].astype(bf16)


def finish_body(sums, *rest):
    xt, (q_out, zs, dq) = rest[:NX], rest[NX:]
    _, _, y, x = position()
    w = [sums[i].astype(f32) for i in range(NY)]
    dq[...] = (((w[0] + w[1]) + (w[2] + w[3])) * SCALE).astype(bf16)
    q_out[...] = dq[pl.ds(pl.multiple_of(y * T, T), T)]
    acc = None
    for i in range(0, NY, 2):
        cols = [jnp.concatenate([xt[d][:, i + e].reshape(T, T) for d in range(NX)], axis=0) for e in range(2)]
        part = nn(jnp.concatenate(cols, axis=1), dq[i * T : (i + 2) * T])
        acc = part if acc is None else acc + part
    for d in range(NX):
        zs[pl.ds(((x - d) % NX) * 4, 4)] = acc[d * T : (d + 1) * T].astype(bf16).reshape(4, 32, H)


def vmem(count):
    return [pl.BlockSpec(memory_space=pltpu.VMEM)] * count


def position():
    return [lax.axis_index(n) for n in ("zp", "zl", "y", "x")]


def call(body, out_shape, scratch, count):
    return pl.pallas_call(
        body,
        in_specs=vmem(count),
        out_specs=tuple(vmem(len(out_shape))),
        out_shape=tuple(jax.ShapeDtypeStruct(s, d) for s, d in out_shape),
        scratch_shapes=scratch,
    )


def per_device(q, k, v, g, lse, o, do, x):
    y = lax.axis_index("y")
    pack = call(pack_body, [((NP, ZB, H), bf16), ((YB, H), bf16)], [], 8)
    zsend, own = pack(q, k, v, g.reshape(1, T), lse.reshape(1, T), o, do, x)
    recv = lax.all_to_all(zsend, ("zp", "zl"), 0, 0, axis_index_groups=GROUPS, tiled=True)
    grp = lax.all_gather(own, "y", axis=0, tiled=False)
    part = [lax.dynamic_slice_in_dim(grp, XB + half * T + y * 32, 32, 1) for half in range(2)]
    xt = lax.all_gather(jnp.concatenate(part, axis=1), "c", axis=0, tiled=False)
    xts = [xt]
    for d in range(1, NX):
        xts.append(lax.ppermute(xt, "x", [(i, (i + d) % NX) for i in range(NX)]))
    recv, *xts[:2] = lax.optimization_barrier((recv, *xts[:2]))
    relayed = lax.ppermute(recv, "zl", [(0, 1), (1, 0)])
    block = (NY * T, H)
    sums = call(first_body, [(block, f32)] * 3, [], 2)(recv, grp)
    second = call(
        last_body,
        [((NY, NY * T, H), bf16)] + [((2 * T, H), bf16)] * NY,
        [pltpu.VMEM(block, f32)] * 3,
        5,
    )
    q_sums, *kv = second(relayed, grp, *sums)
    q_sums = lax.all_to_all(q_sums, "y", 0, 0, tiled=True)
    outs = [((T, H), bf16), ((NZ, 32, H), bf16)]
    finish = call(finish_body, outs, [pltpu.VMEM(block, bf16)], 1 + NX)
    q_grad, zs = finish(q_sums, *xts)
    zs, *kv = lax.optimization_barrier((zs, *kv))
    back = lax.all_to_all(zs, ("zp", "zl"), 0, 0, tiled=True)
    total = kv[0].astype(f32)
    for d in range(1, NY):
        turned = lax.ppermute(kv[d], "y", [(i, (i + d) % NY) for i in range(NY)])
        total = total + turned.astype(f32)
    k_grad = (total[0:T] * SCALE).astype(bf16)
    v_grad = total[T : 2 * T].astype(bf16)
    return q_grad, k_grad, v_grad, jnp.sum(back.astype(f32), axis=0)


def solution(mesh):
    finer = Mesh(mesh.devices.reshape(NP, 2, NY, NX, NC), SP + TP)
    spec = P(SP, TP)
    return jax.shard_map(
        per_device, mesh=finer, in_specs=(spec,) * 8, out_specs=(spec,) * 4, check_vma=False
    )
```

```python
import jax
import jax.numpy as jnp
from jax import lax
from jax.experimental import pallas as pl
from jax.experimental.pallas import tpu as pltpu
from jax.sharding import Mesh
from jax.sharding import PartitionSpec as P

SP = ("zp", "zl", "y")
TP = ("x", "c")
NZ, NP, NY, NX, NC = 16, 8, 4, 4, 2
GROUPS = [[2 * j + (g ^ (j // 4)) for j in range(NP)] for g in range(2)]
T = 128
H = 128
SCALE = H**-0.5
ZB = 2 * T + 8
ST = 4 * T
XB = ST + 16
YB = XB + 2 * T
f32 = jnp.float32
bf16 = jnp.bfloat16


def nt(a, b):
    return lax.dot_general(a, b, (((1,), (1,)), ((), ())), preferred_element_type=f32)


def nn(a, b):
    return lax.dot_general(a, b, (((1,), (0,)), ((), ())), preferred_element_type=f32)


def three(x):
    hi = x.astype(bf16)
    rest = x - hi.astype(f32)
    mid = rest.astype(bf16)
    low = (rest - mid.astype(f32)).astype(bf16)
    return [hi, mid, low]


def pack_body(q, k, v, g, lse, o, do, x, zsend, own):
    zp, zl, _, _ = position()
    terms = o[...].astype(f32) * do[...].astype(f32)
    r = jnp.sum(terms.T, axis=0, keepdims=True)
    gate = g[...]
    a = gate - lse[...]
    zero = jnp.zeros((1, T), bf16)
    q_stats = three(a) + three(r)
    k_stats = three(gate)
    q_rows = jnp.concatenate(q_stats + [zero, zero], axis=0)
    k_rows = jnp.concatenate(k_stats + [zero] * 5, axis=0)
    own[0:T] = q[...]
    own[T : 2 * T] = do[...]
    own[2 * T : 3 * T] = k[...]
    own[3 * T : 4 * T] = v[...]
    own[ST:XB] = jnp.concatenate(q_stats + k_stats + [zero] * 7, axis=0)
    own[XB:YB] = x[...].T

    def one(j, carry):
        up = j + 1 > zp + zl

        @pl.when(up)
        def _():
            zsend[j, 0:T] = k[...]
            zsend[j, T : 2 * T] = v[...]
            zsend[j, 2 * T : ZB] = k_rows

        @pl.when(jnp.logical_not(up))
        def _():
            zsend[j, 0:T] = q[...]
            zsend[j, T : 2 * T] = do[...]
            zsend[j, 2 * T : ZB] = q_rows

        return carry

    lax.fori_loop(0, NP, one, 0)


def joined(rows):
    w = rows.astype(f32)
    return w[0:1] + w[1:2] + w[2:3]


def upright(row):
    i = lax.broadcasted_iota(jnp.int32, (T, T), 0)
    j = lax.broadcasted_iota(jnp.int32, (T, T), 1)
    return jnp.sum(jnp.where(i == j, row, 0.0), axis=1, keepdims=True)


def tall(grp, at):
    return jnp.concatenate([grp[i, at : at + T] for i in range(NY)], axis=0)


def tall_stat(grp, at):
    return jnp.concatenate([upright(joined(grp[i, ST:XB][at : at + 3])) for i in range(NY)], axis=0)


def parts_of(grp):
    qg, dog, kg, vg = (tall(grp, i * T) for i in range(4))
    a_col, r_col, g_col = (tall_stat(grp, 3 * i) for i in range(3))

    def query_part(k, v, g_row, mask=None):
        s = nt(qg, k) * SCALE + (a_col - g_row)
        if mask is not None:
            s = jnp.where(mask, s, -jnp.inf)
        w = jnp.exp(s)
        sl = (w * (nt(dog, v) - r_col)).astype(bf16)
        return nn(sl, k)

    def key_part(q, do, a_row, r_row, mask=None):
        s = nt(kg, q) * SCALE + (a_row - g_col)
        if mask is not None:
            s = jnp.where(mask, s, -jnp.inf)
        w = jnp.exp(s)
        sl = (w * (nt(vg, do) - r_row)).astype(bf16)
        return nn(sl, q), nn(w.astype(bf16), do)

    return query_part, key_part


def received(recv, query_part, key_part, below_end, above_start, dq, dk, dv):
    def block(j, count, at):
        return recv[pl.ds(j, count), at * T : (at + 1) * T].reshape(count * T, H)

    def stat(j, count, at):
        rows = [joined(recv[j + i, 2 * T : ZB][at : at + 3]) for i in range(count)]
        return jnp.concatenate(rows, axis=1)

    def below(j, count):
        dq[...] += query_part(block(j, count, 0), block(j, count, 1), stat(j, count, 0))

    def above(j, count):
        more = key_part(block(j, count, 0), block(j, count, 1), stat(j, count, 0), stat(j, count, 3))
        dk[...] += more[0]
        dv[...] += more[1]

    def over(step, start, end):
        twos = (end - start) // 2

        def two(i, carry):
            step(start + 2 * i, 2)
            return carry

        lax.fori_loop(0, twos, two, 0)

        @pl.when(start + 2 * twos < end)
        def _():
            step(end - 1, 1)

    over(below, 0, below_end)
    over(above, above_start, NP)


def first_body(recv, grp, dq, dk, dv):
    zp, _, y, _ = position()
    query_part, key_part = parts_of(grp)
    big = lax.broadcasted_iota(jnp.int32, (NY * T, T), 0)
    small = lax.broadcasted_iota(jnp.int32, (NY * T, T), 1) + y * T
    st = grp[y, ST:XB]
    dq[...] = query_part(grp[y, 2 * T : 3 * T], grp[y, 3 * T : 4 * T], joined(st[6:9]), small <= big)
    dk[...], dv[...] = key_part(
        grp[y, 0:T], grp[y, T : 2 * T], joined(st[0:3]), joined(st[3:6]), big <= small
    )
    received(recv, query_part, key_part, zp, zp + 1, dq, dk, dv)


def last_body(recv, grp, dq0, dk0, dv0, q_sums, *rest):
    kv_sums, (dq, dk, dv) = rest[:NY], rest[NY:]
    zp, zl, y, _ = position()
    border = zp + zl
    query_part, key_part = parts_of(grp)
    dq[...] = dq0[...]
    dk[...] = dk0[...]
    dv[...] = dv0[...]
    received(recv, query_part, key_part, border, border, dq, dk, dv)
    sums = dq[...].astype(bf16)
    for d in range(NY):
        at = pl.ds(pl.multiple_of(((y + d) % NY) * T, T), T)
        q_sums[d] = sums
        kv_sums[d][0:T] = dk[at].astype(bf16)
        kv_sums[d][T : 2 * T] = dv[at].astype(bf16)


def finish_body(sums, *rest):
    xt, (q_out, zs, dq) = rest[:NX], rest[NX:]
    _, _, y, x = position()
    w = [sums[i].astype(f32) for i in range(NY)]
    dq[...] = (((w[0] + w[1]) + (w[2] + w[3])) * SCALE).astype(bf16)
    q_out[...] = dq[pl.ds(pl.multiple_of(y * T, T), T)]
    acc = None
    for i in range(0, NY, 2):
        cols = [jnp.concatenate([xt[d][:, i + e].reshape(T, T) for d in range(NX)], axis=0) for e in range(2)]
        part = nn(jnp.concatenate(cols, axis=1), dq[i * T : (i + 2) * T])
        acc = part if acc is None else acc + part
    for d in range(NX):
        zs[pl.ds(((x - d) % NX) * 4, 4)] = acc[d * T : (d + 1) * T].astype(bf16).reshape(4, 32, H)


def vmem(count):
    return [pl.BlockSpec(memory_space=pltpu.VMEM)] * count


def position():
    return [lax.axis_index(n) for n in ("zp", "zl", "y", "x")]


def call(body, out_shape, scratch, count):
    return pl.pallas_call(
        body,
        in_specs=vmem(count),
        out_specs=tuple(vmem(len(out_shape))),
        out_shape=tuple(jax.ShapeDtypeStruct(s, d) for s, d in out_shape),
        scratch_shapes=scratch,
    )


def per_device(q, k, v, g, lse, o, do, x):
    y = lax.axis_index("y")
    pack = call(pack_body, [((NP, ZB, H), bf16), ((YB, H), bf16)], [], 8)
    zsend, own = pack(q, k, v, g.reshape(1, T), lse.reshape(1, T), o, do, x)
    recv = lax.all_to_all(zsend, ("zp", "zl"), 0, 0, axis_index_groups=GROUPS, tiled=True)
    grp = lax.all_gather(own, "y", axis=0, tiled=False)
    part = [lax.dynamic_slice_in_dim(grp, XB + half * T + y * 32, 32, 1) for half in range(2)]
    xt = lax.all_gather(jnp.concatenate(part, axis=1), "c", axis=0, tiled=False)
    xts = [xt]
    for d in range(1, NX):
        xts.append(lax.ppermute(xt, "x", [(i, (i + d) % NX) for i in range(NX)]))
    recv, *xts[:3] = lax.optimization_barrier((recv, *xts[:3]))
    relayed = lax.ppermute(recv, "zl", [(0, 1), (1, 0)])
    block = (NY * T, H)
    sums = call(first_body, [(block, f32)] * 3, [], 2)(recv, grp)
    second = call(
        last_body,
        [((NY, NY * T, H), bf16)] + [((2 * T, H), bf16)] * NY,
        [pltpu.VMEM(block, f32)] * 3,
        5,
    )
    q_sums, *kv = second(relayed, grp, *sums)
    turned = []
    q_sums = lax.all_to_all(q_sums, "y", 0, 0, tiled=True)
    for d in range(1, NY):
        turned.append(lax.ppermute(kv[d], "y", [(i, (i + d) % NY) for i in range(NY)]))
    q_sums, *turned[:2] = lax.optimization_barrier((q_sums, *turned[:2]))
    outs = [((T, H), bf16), ((NZ, 32, H), bf16)]
    finish = call(finish_body, outs, [pltpu.VMEM(block, bf16)], 1 + NX)
    q_grad, zs = finish(q_sums, *xts)
    back = lax.all_to_all(zs, ("zp", "zl"), 0, 0, tiled=True)
    parts = [kv[0], *turned]
    k_grad = (sum(p[0:T].astype(f32) for p in parts) * SCALE).astype(bf16)
    v_grad = sum(p[T : 2 * T].astype(f32) for p in parts).astype(bf16)
    return q_grad, k_grad, v_grad, jnp.sum(back.astype(f32), axis=0)


def solution(mesh):
    finer = Mesh(mesh.devices.reshape(NP, 2, NY, NX, NC), SP + TP)
    spec = P(SP, TP)
    return jax.shard_map(
        per_device, mesh=finer, in_specs=(spec,) * 8, out_specs=(spec,) * 4, check_vma=False
    )
```

```python
import jax
import jax.numpy as jnp
from jax import lax
from jax.experimental import pallas as pl
from jax.experimental.pallas import tpu as pltpu
from jax.sharding import Mesh
from jax.sharding import PartitionSpec as P

SP = ("zp", "zl", "y")
TP = ("x", "c")
NZ, NP, NY, NX, NC = 16, 8, 4, 4, 2
GROUPS = [[2 * j + (g ^ (j // 4)) for j in range(NP)] for g in range(2)]
T = 128
H = 128
SCALE = H**-0.5
ZB = 2 * T + 8
ST = 4 * T
XB = ST + 16
YB = XB + 2 * T
f32 = jnp.float32
bf16 = jnp.bfloat16


def nt(a, b):
    return lax.dot_general(a, b, (((1,), (1,)), ((), ())), preferred_element_type=f32)


def nn(a, b):
    return lax.dot_general(a, b, (((1,), (0,)), ((), ())), preferred_element_type=f32)


def three(x):
    hi = x.astype(bf16)
    rest = x - hi.astype(f32)
    mid = rest.astype(bf16)
    low = (rest - mid.astype(f32)).astype(bf16)
    return [hi, mid, low]


def pack_body(q, k, v, g, lse, o, do, x, zsend, own):
    zp, zl, _, _ = position()
    terms = o[...].astype(f32) * do[...].astype(f32)
    r = jnp.sum(terms.T, axis=0, keepdims=True)
    gate = g[...]
    a = gate - lse[...]
    zero = jnp.zeros((1, T), bf16)
    q_stats = three(a) + three(r)
    k_stats = three(gate)
    q_rows = jnp.concatenate(q_stats + [zero, zero], axis=0)
    k_rows = jnp.concatenate(k_stats + [zero] * 5, axis=0)
    own[0:T] = q[...]
    own[T : 2 * T] = do[...]
    own[2 * T : 3 * T] = k[...]
    own[3 * T : 4 * T] = v[...]
    own[ST:XB] = jnp.concatenate(q_stats + k_stats + [zero] * 7, axis=0)
    own[XB:YB] = x[...].T

    def one(j, carry):
        up = j + 1 > zp + zl

        @pl.when(up)
        def _():
            zsend[j, 0:T] = k[...]
            zsend[j, T : 2 * T] = v[...]
            zsend[j, 2 * T : ZB] = k_rows

        @pl.when(jnp.logical_not(up))
        def _():
            zsend[j, 0:T] = q[...]
            zsend[j, T : 2 * T] = do[...]
            zsend[j, 2 * T : ZB] = q_rows

        return carry

    lax.fori_loop(0, NP, one, 0)


def joined(rows):
    w = rows.astype(f32)
    return w[0:1] + w[1:2] + w[2:3]


def upright(row):
    i = lax.broadcasted_iota(jnp.int32, (T, T), 0)
    j = lax.broadcasted_iota(jnp.int32, (T, T), 1)
    return jnp.sum(jnp.where(i == j, row, 0.0), axis=1, keepdims=True)


def tall(grp, at):
    return jnp.concatenate([grp[i, at : at + T] for i in range(NY)], axis=0)


def tall_stat(grp, at):
    return jnp.concatenate([upright(joined(grp[i, ST:XB][at : at + 3])) for i in range(NY)], axis=0)


def parts_of(grp):
    qg, dog, kg, vg = (tall(grp, i * T) for i in range(4))
    a_col, r_col, g_col = (tall_stat(grp, 3 * i) for i in range(3))

    def query_part(k, v, g_row, mask=None):
        s = nt(qg, k) * SCALE + (a_col - g_row)
        if mask is not None:
            s = jnp.where(mask, s, -jnp.inf)
        w = jnp.exp(s)
        sl = (w * (nt(dog, v) - r_col)).astype(bf16)
        return nn(sl, k)

    def key_part(q, do, a_row, r_row, mask=None):
        s = nt(kg, q) * SCALE + (a_row - g_col)
        if mask is not None:
            s = jnp.where(mask, s, -jnp.inf)
        w = jnp.exp(s)
        sl = (w * (nt(vg, do) - r_row)).astype(bf16)
        return nn(sl, q), nn(w.astype(bf16), do)

    return query_part, key_part


def received(recv, query_part, key_part, below_end, above_start, dq, dk, dv):
    def block(j, count, at):
        return recv[pl.ds(j, count), at * T : (at + 1) * T].reshape(count * T, H)

    def stat(j, count, at):
        rows = [joined(recv[j + i, 2 * T : ZB][at : at + 3]) for i in range(count)]
        return jnp.concatenate(rows, axis=1)

    def below(j, count):
        dq[...] += query_part(block(j, count, 0), block(j, count, 1), stat(j, count, 0))

    def above(j, count):
        more = key_part(block(j, count, 0), block(j, count, 1), stat(j, count, 0), stat(j, count, 3))
        dk[...] += more[0]
        dv[...] += more[1]

    def over(step, start, end):
        twos = (end - start) // 2

        def two(i, carry):
            step(start + 2 * i, 2)
            return carry

        lax.fori_loop(0, twos, two, 0)

        @pl.when(start + 2 * twos < end)
        def _():
            step(end - 1, 1)

    over(below, 0, below_end)
    over(above, above_start, NP)


def first_body(recv, grp, dq, dk, dv):
    zp, _, y, _ = position()
    query_part, key_part = parts_of(grp)
    big = lax.broadcasted_iota(jnp.int32, (NY * T, T), 0)
    small = lax.broadcasted_iota(jnp.int32, (NY * T, T), 1) + y * T
    st = grp[y, ST:XB]
    dq[...] = query_part(grp[y, 2 * T : 3 * T], grp[y, 3 * T : 4 * T], joined(st[6:9]), small <= big)
    dk[...], dv[...] = key_part(
        grp[y, 0:T], grp[y, T : 2 * T], joined(st[0:3]), joined(st[3:6]), big <= small
    )
    received(recv, query_part, key_part, zp, zp + 1, dq, dk, dv)


def last_body(recv, grp, dq0, dk0, dv0, q_sums, *rest):
    kv_sums, (dq, dk, dv) = rest[:NY], rest[NY:]
    zp, zl, y, _ = position()
    border = zp + zl
    query_part, key_part = parts_of(grp)
    dq[...] = dq0[...]
    dk[...] = dk0[...]
    dv[...] = dv0[...]
    received(recv, query_part, key_part, border, border, dq, dk, dv)
    sums = dq[...].astype(bf16)
    for d in range(NY):
        at = pl.ds(pl.multiple_of(((y + d) % NY) * T, T), T)
        q_sums[d] = sums
        kv_sums[d][0:T] = dk[at].astype(bf16)
        kv_sums[d][T : 2 * T] = dv[at].astype(bf16)


def finish_body(sums, *rest):
    xt, (q_out, zs, dq) = rest[:NX], rest[NX:]
    _, _, y, x = position()
    w = [sums[i].astype(f32) for i in range(NY)]
    dq[...] = (((w[0] + w[1]) + (w[2] + w[3])) * SCALE).astype(bf16)
    q_out[...] = dq[pl.ds(pl.multiple_of(y * T, T), T)]
    acc = None
    for i in range(0, NY, 2):
        cols = [jnp.concatenate([xt[d][:, i + e].reshape(T, T) for d in range(NX)], axis=0) for e in range(2)]
        part = nn(jnp.concatenate(cols, axis=1), dq[i * T : (i + 2) * T])
        acc = part if acc is None else acc + part
    for d in range(NX):
        zs[pl.ds(((x - d) % NX) * 4, 4)] = acc[d * T : (d + 1) * T].astype(bf16).reshape(4, 32, H)


def vmem(count):
    return [pl.BlockSpec(memory_space=pltpu.VMEM)] * count


def position():
    return [lax.axis_index(n) for n in ("zp", "zl", "y", "x")]


def call(body, out_shape, scratch, count):
    return pl.pallas_call(
        body,
        in_specs=vmem(count),
        out_specs=tuple(vmem(len(out_shape))),
        out_shape=tuple(jax.ShapeDtypeStruct(s, d) for s, d in out_shape),
        scratch_shapes=scratch,
    )


def per_device(q, k, v, g, lse, o, do, x):
    y = lax.axis_index("y")
    pack = call(pack_body, [((NP, ZB, H), bf16), ((YB, H), bf16)], [], 8)
    zsend, own = pack(q, k, v, g.reshape(1, T), lse.reshape(1, T), o, do, x)
    recv = lax.all_to_all(zsend, ("zp", "zl"), 0, 0, axis_index_groups=GROUPS, tiled=True)
    grp = lax.all_gather(own, "y", axis=0, tiled=False)
    part = [lax.dynamic_slice_in_dim(grp, XB + half * T + y * 32, 32, 1) for half in range(2)]
    xt = lax.all_gather(jnp.concatenate(part, axis=1), "c", axis=0, tiled=False)
    recv, xt = lax.optimization_barrier((recv, xt))
    xts = [xt]
    relayed = lax.ppermute(recv, "zl", [(0, 1), (1, 0)])
    for d in range(1, NX):
        xts.append(lax.ppermute(xt, "x", [(i, (i + d) % NX) for i in range(NX)]))
    block = (NY * T, H)
    sums = call(first_body, [(block, f32)] * 3, [], 2)(recv, grp)
    second = call(
        last_body,
        [((NY, NY * T, H), bf16)] + [((2 * T, H), bf16)] * NY,
        [pltpu.VMEM(block, f32)] * 3,
        5,
    )
    q_sums, *kv = second(relayed, grp, *sums)
    q_sums = lax.all_to_all(q_sums, "y", 0, 0, tiled=True)
    q_sums, xts[3] = lax.optimization_barrier((q_sums, xts[3]))
    outs = [((T, H), bf16), ((NZ, 32, H), bf16)]
    finish = call(finish_body, outs, [pltpu.VMEM(block, bf16)], 1 + NX)
    q_grad, zs = finish(q_sums, *xts)
    zs, *kv = lax.optimization_barrier((zs, *kv))
    back = lax.all_to_all(zs, ("zp", "zl"), 0, 0, tiled=True)
    parts = [kv[0]]
    for d in range(1, NY):
        parts.append(lax.ppermute(kv[d], "y", [(i, (i + d) % NY) for i in range(NY)]))
    k_grad = (sum(p[0:T].astype(f32) for p in parts) * SCALE).astype(bf16)
    v_grad = sum(p[T : 2 * T].astype(f32) for p in parts).astype(bf16)
    return q_grad, k_grad, v_grad, jnp.sum(back.astype(f32), axis=0)


def solution(mesh):
    finer = Mesh(mesh.devices.reshape(NP, 2, NY, NX, NC), SP + TP)
    spec = P(SP, TP)
    return jax.shard_map(
        per_device, mesh=finer, in_specs=(spec,) * 8, out_specs=(spec,) * 4, check_vma=False
    )
```

```python
import jax
import jax.numpy as jnp
from jax import lax
from jax.experimental import pallas as pl
from jax.experimental.pallas import tpu as pltpu
from jax.sharding import Mesh
from jax.sharding import PartitionSpec as P

SP = ("zp", "zl", "y")
TP = ("x", "c")
NZ, NP, NY, NX, NC = 16, 8, 4, 4, 2
GROUPS = [[2 * j + (g ^ (j // 4)) for j in range(NP)] for g in range(2)]
T = 128
H = 128
SCALE = H**-0.5
ZB = 2 * T + 8
ST = 4 * T
XB = ST + 16
YB = XB + 2 * T
f32 = jnp.float32
bf16 = jnp.bfloat16


def nt(a, b):
    return lax.dot_general(a, b, (((1,), (1,)), ((), ())), preferred_element_type=f32)


def nn(a, b):
    return lax.dot_general(a, b, (((1,), (0,)), ((), ())), preferred_element_type=f32)


def three(x):
    hi = x.astype(bf16)
    rest = x - hi.astype(f32)
    mid = rest.astype(bf16)
    low = (rest - mid.astype(f32)).astype(bf16)
    return [hi, mid, low]


def pack_body(q, k, v, g, lse, o, do, x, zsend, own):
    zp, zl, _, _ = position()
    terms = o[...].astype(f32) * do[...].astype(f32)
    r = jnp.sum(terms.T, axis=0, keepdims=True)
    gate = g[...]
    a = gate - lse[...]
    zero = jnp.zeros((1, T), bf16)
    q_stats = three(a) + three(r)
    k_stats = three(gate)
    q_rows = jnp.concatenate(q_stats + [zero, zero], axis=0)
    k_rows = jnp.concatenate(k_stats + [zero] * 5, axis=0)
    own[0:T] = q[...]
    own[T : 2 * T] = do[...]
    own[2 * T : 3 * T] = k[...]
    own[3 * T : 4 * T] = v[...]
    own[ST:XB] = jnp.concatenate(q_stats + k_stats + [zero] * 7, axis=0)
    own[XB:YB] = x[...].T

    def one(j, carry):
        up = j + 1 > zp + zl

        @pl.when(up)
        def _():
            zsend[j, 0:T] = k[...]
            zsend[j, T : 2 * T] = v[...]
            zsend[j, 2 * T : ZB] = k_rows

        @pl.when(jnp.logical_not(up))
        def _():
            zsend[j, 0:T] = q[...]
            zsend[j, T : 2 * T] = do[...]
            zsend[j, 2 * T : ZB] = q_rows

        return carry

    lax.fori_loop(0, NP, one, 0)


def joined(rows):
    w = rows.astype(f32)
    return w[0:1] + w[1:2] + w[2:3]


def upright(row):
    i = lax.broadcasted_iota(jnp.int32, (T, T), 0)
    j = lax.broadcasted_iota(jnp.int32, (T, T), 1)
    return jnp.sum(jnp.where(i == j, row, 0.0), axis=1, keepdims=True)


def tall(grp, at):
    return jnp.concatenate([grp[i, at : at + T] for i in range(NY)], axis=0)


def tall_stat(grp, at):
    return jnp.concatenate([upright(joined(grp[i, ST:XB][at : at + 3])) for i in range(NY)], axis=0)


def parts_of(grp):
    qg, dog, kg, vg = (tall(grp, i * T) for i in range(4))
    a_col, r_col, g_col = (tall_stat(grp, 3 * i) for i in range(3))

    def query_part(k, v, g_row, mask=None):
        s = nt(qg, k) * SCALE + (a_col - g_row)
        if mask is not None:
            s = jnp.where(mask, s, -jnp.inf)
        w = jnp.exp(s)
        sl = (w * (nt(dog, v) - r_col)).astype(bf16)
        return nn(sl, k)

    def key_part(q, do, a_row, r_row, mask=None):
        s = nt(kg, q) * SCALE + (a_row - g_col)
        if mask is not None:
            s = jnp.where(mask, s, -jnp.inf)
        w = jnp.exp(s)
        sl = (w * (nt(vg, do) - r_row)).astype(bf16)
        return nn(sl, q), nn(w.astype(bf16), do)

    return query_part, key_part


def received(recv, query_part, key_part, below_end, above_start, dq, dk, dv):
    def block(j, count, at):
        return recv[pl.ds(j, count), at * T : (at + 1) * T].reshape(count * T, H)

    def stat(j, count, at):
        rows = [joined(recv[j + i, 2 * T : ZB][at : at + 3]) for i in range(count)]
        return jnp.concatenate(rows, axis=1)

    def below(j, count):
        dq[...] += query_part(block(j, count, 0), block(j, count, 1), stat(j, count, 0))

    def above(j, count):
        more = key_part(block(j, count, 0), block(j, count, 1), stat(j, count, 0), stat(j, count, 3))
        dk[...] += more[0]
        dv[...] += more[1]

    def over(step, start, end):
        twos = (end - start) // 2

        def two(i, carry):
            step(start + 2 * i, 2)
            return carry

        lax.fori_loop(0, twos, two, 0)

        @pl.when(start + 2 * twos < end)
        def _():
            step(end - 1, 1)

    over(below, 0, below_end)
    over(above, above_start, NP)


def first_body(recv, grp, dq, dk, dv):
    zp, _, y, _ = position()
    query_part, key_part = parts_of(grp)
    big = lax.broadcasted_iota(jnp.int32, (NY * T, T), 0)
    small = lax.broadcasted_iota(jnp.int32, (NY * T, T), 1) + y * T
    st = grp[y, ST:XB]
    dq[...] = query_part(grp[y, 2 * T : 3 * T], grp[y, 3 * T : 4 * T], joined(st[6:9]), small <= big)
    dk[...], dv[...] = key_part(
        grp[y, 0:T], grp[y, T : 2 * T], joined(st[0:3]), joined(st[3:6]), big <= small
    )
    received(recv, query_part, key_part, zp, zp + 1, dq, dk, dv)


def last_body(recv, grp, dq0, dk0, dv0, q_sums, *rest):
    kv_sums, (dq, dk, dv) = rest[:NY], rest[NY:]
    zp, zl, y, _ = position()
    border = zp + zl
    query_part, key_part = parts_of(grp)
    dq[...] = dq0[...]
    dk[...] = dk0[...]
    dv[...] = dv0[...]
    received(recv, query_part, key_part, border, border, dq, dk, dv)
    sums = dq[...].astype(bf16)
    for d in range(NY):
        at = pl.ds(pl.multiple_of(((y + d) % NY) * T, T), T)
        q_sums[d] = sums
        kv_sums[d][0:T] = dk[at].astype(bf16)
        kv_sums[d][T : 2 * T] = dv[at].astype(bf16)


def finish_body(sums, *rest):
    xt, (q_out, zs, dq) = rest[:NX], rest[NX:]
    _, _, y, x = position()
    w = [sums[i].astype(f32) for i in range(NY)]
    dq[...] = (((w[0] + w[1]) + (w[2] + w[3])) * SCALE).astype(bf16)
    q_out[...] = dq[pl.ds(pl.multiple_of(y * T, T), T)]
    acc = None
    for i in range(0, NY, 2):
        cols = [jnp.concatenate([xt[d][:, i + e].reshape(T, T) for d in range(NX)], axis=0) for e in range(2)]
        part = nn(jnp.concatenate(cols, axis=1), dq[i * T : (i + 2) * T])
        acc = part if acc is None else acc + part
    for d in range(NX):
        zs[pl.ds(((x - d) % NX) * 4, 4)] = acc[d * T : (d + 1) * T].astype(bf16).reshape(4, 32, H)


def vmem(count):
    return [pl.BlockSpec(memory_space=pltpu.VMEM)] * count


def in_vmem(a):
    return pltpu.with_memory_space_constraint(a, pltpu.VMEM)


def position():
    return [lax.axis_index(n) for n in ("zp", "zl", "y", "x")]


def call(body, outs, scratch, count, kept=0, limit=16 * 2**20):
    shapes = [pltpu.VMEM(*o) if i >= kept else jax.ShapeDtypeStruct(*o) for i, o in enumerate(outs)]
    return pl.pallas_call(
        body,
        in_specs=vmem(count),
        out_specs=tuple(vmem(len(outs))),
        out_shape=tuple(shapes),
        scratch_shapes=scratch,
        compiler_params=pltpu.CompilerParams(vmem_limit_bytes=limit),
    )


def per_device(q, k, v, g, lse, o, do, x):
    y = lax.axis_index("y")
    pack = call(pack_body, [((NP, ZB, H), bf16), ((YB, H), bf16)], [], 8, limit=60 * 2**20)
    zsend, own = pack(q, k, v, g.reshape(1, T), lse.reshape(1, T), o, do, x)
    recv = lax.all_to_all(zsend, ("zp", "zl"), 0, 0, axis_index_groups=GROUPS, tiled=True)
    grp = lax.all_gather(own, "y", axis=0, tiled=False)
    part = [lax.dynamic_slice_in_dim(grp, XB + half * T + y * 32, 32, 1) for half in range(2)]
    xt = lax.all_gather(jnp.concatenate(part, axis=1), "c", axis=0, tiled=False)
    xts = [xt]
    for d in range(1, NX):
        xts.append(lax.ppermute(xt, "x", [(i, (i + d) % NX) for i in range(NX)]))
    recv, *xts[:2] = lax.optimization_barrier((recv, *xts[:2]))
    relayed = lax.ppermute(recv, "zl", [(0, 1), (1, 0)])
    block = (NY * T, H)
    sums = call(first_body, [(block, f32)] * 3, [], 2)(in_vmem(recv), in_vmem(grp))
    second = call(
        last_body,
        [((NY, NY * T, H), bf16)] + [((2 * T, H), bf16)] * NY,
        [pltpu.VMEM(block, f32)] * 3,
        5,
    )
    q_sums, *kv = second(*[in_vmem(a) for a in (relayed, grp, *sums)])
    q_sums = lax.all_to_all(q_sums, "y", 0, 0, tiled=True)
    outs = [((T, H), bf16), ((NZ, 32, H), bf16)]
    finish = call(finish_body, outs, [pltpu.VMEM(block, bf16)], 1 + NX, kept=1)
    q_grad, zs = finish(in_vmem(q_sums), *[in_vmem(a) for a in xts])
    zs, *kv = lax.optimization_barrier((zs, *kv))
    back = lax.all_to_all(zs, ("zp", "zl"), 0, 0, tiled=True)
    parts = [kv[0]]
    for d in range(1, NY):
        parts.append(lax.ppermute(kv[d], "y", [(i, (i + d) % NY) for i in range(NY)]))
    k_grad = (sum(p[0:T].astype(f32) for p in parts) * SCALE).astype(bf16)
    v_grad = sum(p[T : 2 * T].astype(f32) for p in parts).astype(bf16)
    return q_grad, k_grad, v_grad, jnp.sum(back.astype(f32), axis=0)


def solution(mesh):
    finer = Mesh(mesh.devices.reshape(NP, 2, NY, NX, NC), SP + TP)
    spec = P(SP, TP)
    return jax.shard_map(
        per_device, mesh=finer, in_specs=(spec,) * 8, out_specs=(spec,) * 4, check_vma=False
    )
```

```python
import jax
import jax.numpy as jnp
from jax import lax
from jax.experimental import pallas as pl
from jax.experimental.pallas import tpu as pltpu
from jax.sharding import Mesh
from jax.sharding import PartitionSpec as P

SP = ("zp", "zl", "y")
TP = ("x", "c")
NZ, NP, NY, NX, NC = 16, 8, 4, 4, 2
GROUPS = [[2 * j + (g ^ (j // 4)) for j in range(NP)] for g in range(2)]
T = 128
H = 128
SCALE = H**-0.5
ZB = 2 * T + 8
ST = 4 * T
XB = ST + 16
YB = XB + 2 * T
f32 = jnp.float32
bf16 = jnp.bfloat16


def nt(a, b):
    return lax.dot_general(a, b, (((1,), (1,)), ((), ())), preferred_element_type=f32)


def nn(a, b):
    return lax.dot_general(a, b, (((1,), (0,)), ((), ())), preferred_element_type=f32)


def three(x):
    hi = x.astype(bf16)
    rest = x - hi.astype(f32)
    mid = rest.astype(bf16)
    low = (rest - mid.astype(f32)).astype(bf16)
    return [hi, mid, low]


def pack_body(q, k, v, g, lse, o, do, x, zsend, own):
    zp, zl, _, _ = position()
    terms = o[...].astype(f32) * do[...].astype(f32)
    r = jnp.sum(terms.T, axis=0, keepdims=True)
    gate = g[...]
    a = gate - lse[...]
    zero = jnp.zeros((1, T), bf16)
    q_stats = three(a) + three(r)
    k_stats = three(gate)
    q_rows = jnp.concatenate(q_stats + [zero, zero], axis=0)
    k_rows = jnp.concatenate(k_stats + [zero] * 5, axis=0)
    own[0:T] = q[...]
    own[T : 2 * T] = do[...]
    own[2 * T : 3 * T] = k[...]
    own[3 * T : 4 * T] = v[...]
    own[ST:XB] = jnp.concatenate(q_stats + k_stats + [zero] * 7, axis=0)
    own[XB:YB] = x[...].T

    def one(j, carry):
        up = j + 1 > zp + zl

        @pl.when(up)
        def _():
            zsend[j, 0:T] = k[...]
            zsend[j, T : 2 * T] = v[...]
            zsend[j, 2 * T : ZB] = k_rows

        @pl.when(jnp.logical_not(up))
        def _():
            zsend[j, 0:T] = q[...]
            zsend[j, T : 2 * T] = do[...]
            zsend[j, 2 * T : ZB] = q_rows

        return carry

    lax.fori_loop(0, NP, one, 0)


def joined(rows):
    w = rows.astype(f32)
    return w[0:1] + w[1:2] + w[2:3]


def upright(row):
    i = lax.broadcasted_iota(jnp.int32, (T, T), 0)
    j = lax.broadcasted_iota(jnp.int32, (T, T), 1)
    return jnp.sum(jnp.where(i == j, row, 0.0), axis=1, keepdims=True)


def tall(grp, at):
    return jnp.concatenate([grp[i, at : at + T] for i in range(NY)], axis=0)


def tall_stat(grp, at):
    return jnp.concatenate([upright(joined(grp[i, ST:XB][at : at + 3])) for i in range(NY)], axis=0)


def parts_of(grp):
    qg, dog, kg, vg = (tall(grp, i * T) for i in range(4))
    a_col, r_col, g_col = (tall_stat(grp, 3 * i) for i in range(3))

    def query_part(k, v, g_row, mask=None):
        s = nt(qg, k) * SCALE + (a_col - g_row)
        if mask is not None:
            s = jnp.where(mask, s, -jnp.inf)
        w = jnp.exp(s)
        sl = (w * (nt(dog, v) - r_col)).astype(bf16)
        return nn(sl, k)

    def key_part(q, do, a_row, r_row, mask=None):
        s = nt(kg, q) * SCALE + (a_row - g_col)
        if mask is not None:
            s = jnp.where(mask, s, -jnp.inf)
        w = jnp.exp(s)
        sl = (w * (nt(vg, do) - r_row)).astype(bf16)
        return nn(sl, q), nn(w.astype(bf16), do)

    return query_part, key_part


def received(recv, query_part, key_part, below_end, above_start, dq, dk, dv):
    def block(j, count, at):
        return recv[pl.ds(j, count), at * T : (at + 1) * T].reshape(count * T, H)

    def stat(j, count, at):
        rows = [joined(recv[j + i, 2 * T : ZB][at : at + 3]) for i in range(count)]
        return jnp.concatenate(rows, axis=1)

    def below(j, count):
        dq[...] += query_part(block(j, count, 0), block(j, count, 1), stat(j, count, 0))

    def above(j, count):
        more = key_part(block(j, count, 0), block(j, count, 1), stat(j, count, 0), stat(j, count, 3))
        dk[...] += more[0]
        dv[...] += more[1]

    def over(step, start, end):
        fours = (end - start) // 4

        def four(i, carry):
            step(start + 4 * i, 4)
            return carry

        lax.fori_loop(0, fours, four, 0)
        left = (end - start) % 4

        @pl.when(left >= 2)
        def _():
            step(start + 4 * fours, 2)

        @pl.when(left % 2 == 1)
        def _():
            step(end - 1, 1)

    over(below, 0, below_end)
    over(above, above_start, NP)


def first_body(recv, grp, dq, dk, dv):
    zp, _, y, _ = position()
    query_part, key_part = parts_of(grp)
    big = lax.broadcasted_iota(jnp.int32, (NY * T, T), 0)
    small = lax.broadcasted_iota(jnp.int32, (NY * T, T), 1) + y * T
    st = grp[y, ST:XB]
    dq[...] = query_part(grp[y, 2 * T : 3 * T], grp[y, 3 * T : 4 * T], joined(st[6:9]), small <= big)
    dk[...], dv[...] = key_part(
        grp[y, 0:T], grp[y, T : 2 * T], joined(st[0:3]), joined(st[3:6]), big <= small
    )
    received(recv, query_part, key_part, zp, zp + 1, dq, dk, dv)


def last_body(recv, grp, dq0, dk0, dv0, q_sums, *rest):
    kv_sums, (dq, dk, dv) = rest[:NY], rest[NY:]
    zp, zl, y, _ = position()
    border = zp + zl
    query_part, key_part = parts_of(grp)
    dq[...] = dq0[...]
    dk[...] = dk0[...]
    dv[...] = dv0[...]
    received(recv, query_part, key_part, border, border, dq, dk, dv)
    sums = dq[...].astype(bf16)
    for d in range(NY):
        at = pl.ds(pl.multiple_of(((y + d) % NY) * T, T), T)
        q_sums[d] = sums
        kv_sums[d][0:T] = dk[at].astype(bf16)
        kv_sums[d][T : 2 * T] = dv[at].astype(bf16)


def finish_body(sums, *rest):
    xt, (q_out, zs, dq) = rest[:NX], rest[NX:]
    _, _, y, x = position()
    w = [sums[i].astype(f32) for i in range(NY)]
    dq[...] = (((w[0] + w[1]) + (w[2] + w[3])) * SCALE).astype(bf16)
    q_out[...] = dq[pl.ds(pl.multiple_of(y * T, T), T)]
    acc = None
    for i in range(0, NY, 2):
        cols = [jnp.concatenate([xt[d][:, i + e].reshape(T, T) for d in range(NX)], axis=0) for e in range(2)]
        part = nn(jnp.concatenate(cols, axis=1), dq[i * T : (i + 2) * T])
        acc = part if acc is None else acc + part
    for d in range(NX):
        zs[pl.ds(((x - d) % NX) * 4, 4)] = acc[d * T : (d + 1) * T].astype(bf16).reshape(4, 32, H)


def vmem(count):
    return [pl.BlockSpec(memory_space=pltpu.VMEM)] * count


def in_vmem(a):
    return pltpu.with_memory_space_constraint(a, pltpu.VMEM)


def position():
    return [lax.axis_index(n) for n in ("zp", "zl", "y", "x")]


def call(body, outs, scratch, count, kept=0, limit=16 * 2**20):
    shapes = [pltpu.VMEM(*o) if i >= kept else jax.ShapeDtypeStruct(*o) for i, o in enumerate(outs)]
    return pl.pallas_call(
        body,
        in_specs=vmem(count),
        out_specs=tuple(vmem(len(outs))),
        out_shape=tuple(shapes),
        scratch_shapes=scratch,
        compiler_params=pltpu.CompilerParams(vmem_limit_bytes=limit),
    )


def per_device(q, k, v, g, lse, o, do, x):
    y = lax.axis_index("y")
    pack = call(pack_body, [((NP, ZB, H), bf16), ((YB, H), bf16)], [], 8, limit=60 * 2**20)
    zsend, own = pack(q, k, v, g.reshape(1, T), lse.reshape(1, T), o, do, x)
    recv = lax.all_to_all(zsend, ("zp", "zl"), 0, 0, axis_index_groups=GROUPS, tiled=True)
    grp = lax.all_gather(own, "y", axis=0, tiled=False)
    part = [lax.dynamic_slice_in_dim(grp, XB + half * T + y * 32, 32, 1) for half in range(2)]
    xt = lax.all_gather(jnp.concatenate(part, axis=1), "c", axis=0, tiled=False)
    xts = [xt]
    for d in range(1, NX):
        xts.append(lax.ppermute(xt, "x", [(i, (i + d) % NX) for i in range(NX)]))
    recv, xts[0] = lax.optimization_barrier((recv, xts[0]))
    relayed = lax.ppermute(recv, "zl", [(0, 1), (1, 0)])
    block = (NY * T, H)
    sums = call(first_body, [(block, f32)] * 3, [], 2)(in_vmem(recv), in_vmem(grp))
    second = call(
        last_body,
        [((NY, NY * T, H), bf16)] + [((2 * T, H), bf16)] * NY,
        [pltpu.VMEM(block, f32)] * 3,
        5,
    )
    q_sums, *kv = second(*[in_vmem(a) for a in (relayed, grp, *sums)])
    q_sums = lax.all_to_all(q_sums, "y", 0, 0, tiled=True)
    outs = [((T, H), bf16), ((NZ, 32, H), bf16)]
    finish = call(finish_body, outs, [pltpu.VMEM(block, bf16)], 1 + NX, kept=1)
    q_grad, zs = finish(in_vmem(q_sums), *[in_vmem(a) for a in xts])
    zs, *kv = lax.optimization_barrier((zs, *kv))
    back = lax.all_to_all(zs, ("zp", "zl"), 0, 0, tiled=True)
    parts = [kv[0]]
    for d in range(1, NY):
        parts.append(lax.ppermute(kv[d], "y", [(i, (i + d) % NY) for i in range(NY)]))
    k_grad = (sum(p[0:T].astype(f32) for p in parts) * SCALE).astype(bf16)
    v_grad = sum(p[T : 2 * T].astype(f32) for p in parts).astype(bf16)
    return q_grad, k_grad, v_grad, jnp.sum(back.astype(f32), axis=0)


def solution(mesh):
    finer = Mesh(mesh.devices.reshape(NP, 2, NY, NX, NC), SP + TP)
    spec = P(SP, TP)
    return jax.shard_map(
        per_device, mesh=finer, in_specs=(spec,) * 8, out_specs=(spec,) * 4, check_vma=False
    )
```

```python
import jax
import jax.numpy as jnp
from jax import lax
from jax.experimental import pallas as pl
from jax.experimental.pallas import tpu as pltpu
from jax.sharding import Mesh
from jax.sharding import PartitionSpec as P

SP = ("zp", "zl", "y")
TP = ("x", "c")
NZ, NP, NY, NX, NC = 16, 8, 4, 4, 2
GROUPS = [[2 * j + (g ^ (j // 4)) for j in range(NP)] for g in range(2)]
T = 128
H = 128
SCALE = H**-0.5
ZB = 2 * T + 8
ST = 4 * T
XB = ST + 16
YB = XB + 2 * T
f32 = jnp.float32
bf16 = jnp.bfloat16


def nt(a, b):
    return lax.dot_general(a, b, (((1,), (1,)), ((), ())), preferred_element_type=f32)


def nn(a, b):
    return lax.dot_general(a, b, (((1,), (0,)), ((), ())), preferred_element_type=f32)


def three(x):
    hi = x.astype(bf16)
    rest = x - hi.astype(f32)
    mid = rest.astype(bf16)
    low = (rest - mid.astype(f32)).astype(bf16)
    return [hi, mid, low]


def pack_body(q, k, v, g, lse, o, do, x, zsend, own):
    zp, zl, _, _ = position()
    terms = o[...].astype(f32) * do[...].astype(f32)
    r = jnp.sum(terms.T, axis=0, keepdims=True)
    gate = g[...]
    a = gate - lse[...]
    zero = jnp.zeros((1, T), bf16)
    q_stats = three(a) + three(r)
    k_stats = three(gate)
    q_rows = jnp.concatenate(q_stats + [zero, zero], axis=0)
    k_rows = jnp.concatenate(k_stats + [zero] * 5, axis=0)
    own[0:T] = q[...]
    own[T : 2 * T] = do[...]
    own[2 * T : 3 * T] = k[...]
    own[3 * T : 4 * T] = v[...]
    own[ST:XB] = jnp.concatenate(q_stats + k_stats + [zero] * 7, axis=0)
    own[XB:YB] = x[...].T

    def one(j, carry):
        up = j + 1 > zp + zl

        @pl.when(up)
        def _():
            zsend[j, 0:T] = k[...]
            zsend[j, T : 2 * T] = v[...]
            zsend[j, 2 * T : ZB] = k_rows

        @pl.when(jnp.logical_not(up))
        def _():
            zsend[j, 0:T] = q[...]
            zsend[j, T : 2 * T] = do[...]
            zsend[j, 2 * T : ZB] = q_rows

        return carry

    lax.fori_loop(0, NP, one, 0)


def joined(rows):
    w = rows.astype(f32)
    return w[0:1] + w[1:2] + w[2:3]


def upright(row):
    i = lax.broadcasted_iota(jnp.int32, (T, T), 0)
    j = lax.broadcasted_iota(jnp.int32, (T, T), 1)
    return jnp.sum(jnp.where(i == j, row, 0.0), axis=1, keepdims=True)


def tall(grp, at):
    return jnp.concatenate([grp[i, at : at + T] for i in range(NY)], axis=0)


def tall_stat(grp, at):
    return jnp.concatenate([upright(joined(grp[i, ST:XB][at : at + 3])) for i in range(NY)], axis=0)


def parts_of(grp):
    qg, dog, kg, vg = (tall(grp, i * T) for i in range(4))
    a_col, r_col, g_col = (tall_stat(grp, 3 * i) for i in range(3))

    def query_part(k, v, g_row, mask=None):
        s = nt(qg, k) * SCALE + (a_col - g_row)
        if mask is not None:
            s = jnp.where(mask, s, -jnp.inf)
        w = jnp.exp(s)
        sl = (w * (nt(dog, v) - r_col)).astype(bf16)
        return nn(sl, k)

    def key_part(q, do, a_row, r_row, mask=None):
        s = nt(kg, q) * SCALE + (a_row - g_col)
        if mask is not None:
            s = jnp.where(mask, s, -jnp.inf)
        w = jnp.exp(s)
        sl = (w * (nt(vg, do) - r_row)).astype(bf16)
        return nn(sl, q), nn(w.astype(bf16), do)

    return query_part, key_part


def received(recv, query_part, key_part, below_end, above_start, dq, dk, dv):
    def block(j, count, at):
        return recv[pl.ds(j, count), at * T : (at + 1) * T].reshape(count * T, H)

    def stat(j, count, at):
        rows = [joined(recv[j + i, 2 * T : ZB][at : at + 3]) for i in range(count)]
        return jnp.concatenate(rows, axis=1)

    def below(j, count):
        dq[...] += query_part(block(j, count, 0), block(j, count, 1), stat(j, count, 0))

    def above(j, count):
        more = key_part(block(j, count, 0), block(j, count, 1), stat(j, count, 0), stat(j, count, 3))
        dk[...] += more[0]
        dv[...] += more[1]

    def over(step, start, end):
        eights = (end - start) // NP

        @pl.when(eights == 1)
        def _():
            step(0, NP)

        start = start + NP * eights
        fours = (end - start) // 4

        def four(i, carry):
            step(start + 4 * i, 4)
            return carry

        lax.fori_loop(0, fours, four, 0)
        left = (end - start) % 4

        @pl.when(left >= 2)
        def _():
            step(start + 4 * fours, 2)

        @pl.when(left % 2 == 1)
        def _():
            step(end - 1, 1)

    over(below, 0, below_end)
    over(above, above_start, NP)


def first_body(recv, grp, dq, dk, dv):
    zp, _, y, _ = position()
    query_part, key_part = parts_of(grp)
    big = lax.broadcasted_iota(jnp.int32, (NY * T, T), 0)
    small = lax.broadcasted_iota(jnp.int32, (NY * T, T), 1) + y * T
    st = grp[y, ST:XB]
    dq[...] = query_part(grp[y, 2 * T : 3 * T], grp[y, 3 * T : 4 * T], joined(st[6:9]), small <= big)
    dk[...], dv[...] = key_part(
        grp[y, 0:T], grp[y, T : 2 * T], joined(st[0:3]), joined(st[3:6]), big <= small
    )
    received(recv, query_part, key_part, zp, zp + 1, dq, dk, dv)


def last_body(recv, grp, dq0, dk0, dv0, q_sums, *rest):
    kv_sums, (dq, dk, dv) = rest[:NY], rest[NY:]
    zp, zl, y, _ = position()
    border = zp + zl
    query_part, key_part = parts_of(grp)
    dq[...] = dq0[...]
    dk[...] = dk0[...]
    dv[...] = dv0[...]
    received(recv, query_part, key_part, border, border, dq, dk, dv)
    sums = dq[...].astype(bf16)
    for d in range(NY):
        at = pl.ds(pl.multiple_of(((y + d) % NY) * T, T), T)
        q_sums[d] = sums
        kv_sums[d][0:T] = dk[at].astype(bf16)
        kv_sums[d][T : 2 * T] = dv[at].astype(bf16)


def finish_body(sums, *rest):
    xt, (q_out, zs, dq) = rest[:NX], rest[NX:]
    _, _, y, x = position()
    w = [sums[i].astype(f32) for i in range(NY)]
    dq[...] = (((w[0] + w[1]) + (w[2] + w[3])) * SCALE).astype(bf16)
    q_out[...] = dq[pl.ds(pl.multiple_of(y * T, T), T)]
    acc = None
    for i in range(0, NY, 2):
        cols = [jnp.concatenate([xt[d][:, i + e].reshape(T, T) for d in range(NX)], axis=0) for e in range(2)]
        part = nn(jnp.concatenate(cols, axis=1), dq[i * T : (i + 2) * T])
        acc = part if acc is None else acc + part
    for d in range(NX):
        zs[pl.ds(((x - d) % NX) * 4, 4)] = acc[d * T : (d + 1) * T].astype(bf16).reshape(4, 32, H)


def vmem(count):
    return [pl.BlockSpec(memory_space=pltpu.VMEM)] * count


def in_vmem(a):
    return pltpu.with_memory_space_constraint(a, pltpu.VMEM)


def position():
    return [lax.axis_index(n) for n in ("zp", "zl", "y", "x")]


def call(body, outs, scratch, count, kept=0, limit=16 * 2**20):
    shapes = [pltpu.VMEM(*o) if i >= kept else jax.ShapeDtypeStruct(*o) for i, o in enumerate(outs)]
    return pl.pallas_call(
        body,
        in_specs=vmem(count),
        out_specs=tuple(vmem(len(outs))),
        out_shape=tuple(shapes),
        scratch_shapes=scratch,
        compiler_params=pltpu.CompilerParams(vmem_limit_bytes=limit),
    )


def per_device(q, k, v, g, lse, o, do, x):
    y = lax.axis_index("y")
    pack = call(pack_body, [((NP, ZB, H), bf16), ((YB, H), bf16)], [], 8, limit=60 * 2**20)
    zsend, own = pack(q, k, v, g.reshape(1, T), lse.reshape(1, T), o, do, x)
    recv = lax.all_to_all(zsend, ("zp", "zl"), 0, 0, axis_index_groups=GROUPS, tiled=True)
    grp = lax.all_gather(own, "y", axis=0, tiled=False)
    part = [lax.dynamic_slice_in_dim(grp, XB + half * T + y * 32, 32, 1) for half in range(2)]
    xt = lax.all_gather(jnp.concatenate(part, axis=1), "c", axis=0, tiled=False)
    xts = [xt]
    for d in range(1, NX):
        xts.append(lax.ppermute(xt, "x", [(i, (i + d) % NX) for i in range(NX)]))
    recv, *xts[:2] = lax.optimization_barrier((recv, *xts[:2]))
    relayed = lax.ppermute(recv, "zl", [(0, 1), (1, 0)])
    block = (NY * T, H)
    sums = call(first_body, [(block, f32)] * 3, [], 2)(in_vmem(recv), in_vmem(grp))
    second = call(
        last_body,
        [((NY, NY * T, H), bf16)] + [((2 * T, H), bf16)] * NY,
        [pltpu.VMEM(block, f32)] * 3,
        5,
    )
    q_sums, *kv = second(*[in_vmem(a) for a in (relayed, grp, *sums)])
    q_sums = lax.all_to_all(q_sums, "y", 0, 0, tiled=True)
    outs = [((T, H), bf16), ((NZ, 32, H), bf16)]
    finish = call(finish_body, outs, [pltpu.VMEM(block, bf16)], 1 + NX, kept=1)
    q_grad, zs = finish(in_vmem(q_sums), *[in_vmem(a) for a in xts])
    zs, *kv = lax.optimization_barrier((zs, *kv))
    back = lax.all_to_all(zs, ("zp", "zl"), 0, 0, tiled=True)
    parts = [kv[0]]
    for d in range(1, NY):
        parts.append(lax.ppermute(kv[d], "y", [(i, (i + d) % NY) for i in range(NY)]))
    k_grad = (sum(p[0:T].astype(f32) for p in parts) * SCALE).astype(bf16)
    v_grad = sum(p[T : 2 * T].astype(f32) for p in parts).astype(bf16)
    return q_grad, k_grad, v_grad, jnp.sum(back.astype(f32), axis=0)


def solution(mesh):
    finer = Mesh(mesh.devices.reshape(NP, 2, NY, NX, NC), SP + TP)
    spec = P(SP, TP)
    return jax.shard_map(
        per_device, mesh=finer, in_specs=(spec,) * 8, out_specs=(spec,) * 4, check_vma=False
    )
```
